512 devices in a mesh: ep: 16 (over y, x), tp: 32 (over z, core).
Axes of the slice: x: 4, y: 4, z: 16, core: 2. Of those that a mesh axis runs over, the one named last changes fastest.
Arguments:
- tokens: bfloat16 [2048, 2048], P('ep'), may hold values from -32 to 32
- routes: int32 [2048, 2], P('ep'), may hold values from 0 to 15, all different within a row; in each aligned block of 128 rows (0 to 127, 128 to 255, ...) at most 24 rows name the same one
- gates: float32 [2048, 2], P('ep'), may hold values from 0.05 to 0.6
- cotangent: bfloat16 [2048, 2048], P('ep'), may hold values from -6 to 6
- w_glu: bfloat16 [16, 2048, 1024], P('ep', None, 'tp'), may hold values from -0.125 to 0.125
- w_lin: bfloat16 [16, 2048, 1024], P('ep', None, 'tp'), may hold values from -0.125 to 0.125
- w_down: bfloat16 [16, 1024, 2048], P('ep', 'tp'), may hold values from -0.1875 to 0.1875
Outputs:
- d_tokens: bfloat16 [2048, 2048], P('ep', 'tp')
- d_gates: float32 [2048, 2], P('ep')
- glu_wgrad: float32 [16, 2048, 1024], P('ep', None, 'tp')
- lin_wgrad: float32 [16, 2048, 1024], P('ep', None, 'tp')
- down_wgrad: float32 [16, 1024, 2048], P('ep', 'tp')
- glu_norms: float32 [16, 2048], P('ep')
- lin_norms: float32 [16, 2048], P('ep')
- down_norms: float32 [16, 1024], P('ep', 'tp')
The draws below stay inside these ranges and needn't reach their ends.
Inputs may be any that keep to these rules, and one draw needn't show every extreme that they name: `routes`: each row names 2 different experts. Among the 128 tokens of one aligned block no expert is named more than 24 times, and in every draw some expert is named exactly 24 times in some block.
All inputs are finite; a program needn't handle non-finite values.
Results may differ from the reference program's by a relative error of at most 0.024.
Values may be sent and summed in bfloat16 or wider, within the bound.
No kernel may reach another device: no remote copies, remote signals or barrier semaphores. Data moves between devices by JAX's collectives and lax.ppermute only.
A program may use at most 64 MiB of HBM per device.

```python
import math
import jax
import jax.numpy as jnp
import numpy as np
from jax import lax

D = 2048
F = 1024
TOP = 2
TOK_DEV = 128
EXPERTS = 16
CAP = 24
TOKENS = 2048
N_EP = 16
N_TP = 32


def draw_tokens(key, part):
    first_key, second_key, third_key = jax.random.split(key, 3)
    values = jnp.clip(jax.random.normal(first_key, (TOKENS, D), jnp.float32), -4.0, 4.0)
    return values.astype(jnp.bfloat16)


def steps_of(key, extent, cuts, least, largest):
    loudness = 1.0
    for axis_at, shards_of in cuts:
        steps = jax.random.uniform(jax.random.fold_in(jax.random.fold_in(key, 6), axis_at), (shards_of,), jnp.float32, least / len(cuts), largest / len(cuts))
        loudness = loudness * jnp.repeat(jnp.exp(steps), extent[axis_at] // shards_of).reshape((-1,) + (1,) * (len(extent) - 1 - axis_at))
    return loudness


def routed_block(own_key, own, number, rows, number_of, top, reach, slope):
    sequence = jax.random.permutation(own_key, number_of)
    packed, common = portions_of(number_of, rows * top, reach, slope, True), portions_of(number_of, rows * top, reach, slope, False)
    places = jnp.arange(number_of)

    def named(sizes, turn):
        used = int((sizes > 0).sum())
        fixed = max(1, used // 4)
        shifted = fixed + (places - fixed + turn * (used - fixed)) % max(1, number_of - fixed)
        return jnp.zeros((number_of,), jnp.int32).at[sequence[jnp.where(places < fixed, places, shifted)]].set(jnp.asarray(sizes, jnp.int32))

    sizes = jnp.where(number % 4 == 0, named(packed, number // 4), named(common, number - number // 4 - 1))
    mixed = jax.random.permutation(jax.random.fold_in(own, 3), number_of)
    source_of, sink = mixed[0:number_of // 2 * 2:2], mixed[1:number_of // 2 * 2:2]
    margin = jnp.minimum(sizes[source_of] - 1, reach - sizes[sink]) // 2
    margin = jnp.where((source_of == sequence[0]) | (sink == sequence[0]) | (sizes[sink] == 0), 0, jnp.maximum(margin, 0))
    shifted = jax.random.randint(jax.random.fold_in(own, 4), (number_of // 2,), 0, 1 << 20) % (margin + 1)
    sizes = sizes.at[source_of].add(-shifted).at[sink].add(shifted)
    members = jnp.searchsorted(jnp.cumsum(sizes), jnp.arange(rows * top), side="right").astype(jnp.int32)
    listing = members.reshape(top, rows).T
    listing = listing[jax.random.permutation(jax.random.fold_in(own, 1), rows)]
    turn = jax.random.randint(jax.random.fold_in(own, 2), (rows, 1), 0, top)
    return jnp.take_along_axis(listing, (jnp.arange(top)[None, :] + turn) % top, axis=1)


def portions_of(count, total, most, lean, full):
    portions = [(1 << 20) // math.isqrt(grade ** lean) + 1 for grade in range(1, count + 1)]
    largest = most if full else min(most, max(-(-total // count), total * portions[0] // sum(portions)))
    least = 1 if total - largest >= count - 1 else 0
    counts, spare = [largest] + [least] * (count - 1), total - largest - least * (count - 1)
    while spare > 0:
        candidates = [i for i in range(1, count) if counts[i] < largest] or [i for i in range(1, count) if counts[i] < most]
        mass, left = sum([portions[i] for i in candidates]), spare
        for i in candidates:
            addition = min(most - counts[i], max(1, left * portions[i] // mass), spare)
            counts[i] = counts[i] + addition
            spare = spare - addition
    return np.array(counts)


def normal_values(own_key, dims, deviation, bound, shards=(), kind=jnp.bfloat16):
    array = deviation * jax.random.normal(own_key, dims, jnp.float32)
    if shards:
        array = array * steps_of(own_key, dims, shards, -0.22, 0.18)
    return jnp.clip(array, -bound, bound).astype(kind)


def setup_inputs(seed: int = 0) -> dict:
    streams_of = jax.random.split(jax.random.key(seed), 8)
    tokens = draw_tokens(jax.random.fold_in(streams_of[7], 71), 0)
    routes_keys = jax.random.split(jax.random.fold_in(streams_of[1], 1), TOKENS // TOK_DEV)
    routes_turns = jax.random.permutation(jax.random.fold_in(streams_of[1], 3), TOKENS // TOK_DEV)
    routes = jax.vmap(lambda own, number: routed_block(jax.random.fold_in(streams_of[1], 2), own, number, TOK_DEV, EXPERTS, TOP, CAP, 2))(routes_keys, routes_turns).reshape((TOKENS, TOP))
    gates = jnp.clip(jnp.exp(math.log(0.6) - 2.4849067 * jax.random.uniform(streams_of[2], (TOKENS, TOP), jnp.float32) ** steps_of(streams_of[2], (TOKENS, TOP), ((0, 16),), -0.2, 0.2)), 0.05, 0.6)
    cotangent = normal_values(streams_of[3], (TOKENS, D), 1.0, 6.0, ((0, 16),))
    w_glu = normal_values(streams_of[4], (EXPERTS, D, F), D ** -0.5, 0.125, ((0, 16), (2, 32)))
    w_lin = normal_values(streams_of[5], (EXPERTS, D, F), D ** -0.5, 0.125, ((0, 16), (2, 32)))
    w_down = normal_values(streams_of[6], (EXPERTS, F, D), F ** -0.5, 0.1875, ((0, 16), (1, 32)))
    return {"tokens": tokens, "routes": routes, "gates": gates, "cotangent": cotangent, "w_glu": w_glu, "w_lin": w_lin, "w_down": w_down}


clamp_limit = 7.0
sigmoid_scale = 1.702


def slot_rank(pair_expert, all_experts):
    onehot = (pair_expert[:, None] == jnp.arange(all_experts, dtype=jnp.int32)[None, :]).astype(jnp.int32)
    return (jnp.sum(jnp.cumsum(onehot, axis=0) * onehot, axis=1) - 1).astype(jnp.int32)


def clamp_backward(glu_pre, lin_pre, back_proj, gate_col):
    glu_clip = jnp.minimum(glu_pre, clamp_limit)
    lin_clip = jnp.clip(lin_pre, -clamp_limit, clamp_limit)
    sig_val = jax.nn.sigmoid(sigmoid_scale * glu_clip)
    glu_act = glu_clip * sig_val
    hidden = glu_act * (lin_clip + 1.0)
    hid_grad = gate_col * back_proj
    act_slope = sig_val + sigmoid_scale * glu_clip * sig_val * (1.0 - sig_val)
    glu_grad = jnp.where(glu_pre < clamp_limit, hid_grad * (lin_clip + 1.0) * act_slope, 0.0)
    lin_grad = jnp.where(jnp.abs(lin_pre) < clamp_limit, hid_grad * glu_act, 0.0)
    return hidden, glu_grad.astype(jnp.bfloat16), lin_grad.astype(jnp.bfloat16)


def expert_grads(tok_rows, cot_rows, gate_col, glu_w, lin_w, down_w):
    glu_pre = jnp.dot(tok_rows, glu_w, preferred_element_type=jnp.float32)
    lin_pre = jnp.dot(tok_rows, lin_w, preferred_element_type=jnp.float32)
    back_proj = jnp.dot(cot_rows, down_w.T, preferred_element_type=jnp.float32)
    hidden, glu_bf, lin_bf = clamp_backward(glu_pre, lin_pre, back_proj, gate_col)
    gate_part = jnp.sum(back_proj * hidden, axis=1)
    hidden_gated = (gate_col * hidden).astype(jnp.bfloat16)
    down_wgrad = jnp.dot(hidden_gated.T, cot_rows, preferred_element_type=jnp.float32)
    glu_wgrad = jnp.dot(tok_rows.T, glu_bf, preferred_element_type=jnp.float32)
    lin_wgrad = jnp.dot(tok_rows.T, lin_bf, preferred_element_type=jnp.float32)
    return gate_part, glu_bf, lin_bf, glu_wgrad, lin_wgrad, down_wgrad


def rank_block(block_row):
    return slot_rank(block_row, EXPERTS)


def reference(tokens, routes, gates, cotangent, w_glu, w_lin, w_down):
    pair_count = TOK_DEV * TOP
    slot_total = N_EP * CAP
    block_width = F // N_TP
    block_experts = routes.reshape(N_EP, pair_count)
    ranks = jax.vmap(rank_block)(block_experts)
    sources = jnp.arange(N_EP, dtype=jnp.int32)[:, None] * CAP
    slot_index = (block_experts * slot_total + sources + ranks).reshape(-1).astype(jnp.int32)
    slot_pair = jnp.full((EXPERTS * slot_total,), TOKENS * TOP, jnp.int32).at[slot_index].set(
        jnp.arange(TOKENS * TOP, dtype=jnp.int32)).reshape(EXPERTS, slot_total)
    slot_token = (slot_pair // TOP).astype(jnp.int32)
    tok_ext = jnp.concatenate([tokens, jnp.zeros((1, D), jnp.bfloat16)], axis=0)
    cot_ext = jnp.concatenate([cotangent, jnp.zeros((1, D), jnp.bfloat16)], axis=0)
    gate_ext = jnp.concatenate([gates.reshape(-1), jnp.zeros((1,), jnp.float32)])

    def one_expert(inputs):
        token_ids, pair_ids, glu_w, lin_w, down_w = inputs
        tok_rows = tok_ext[token_ids]
        cot_rows = cot_ext[token_ids]
        gate_col = gate_ext[pair_ids][:, None]
        gate_part, glu_bf, lin_bf, glu_wgrad, lin_wgrad, down_wgrad = expert_grads(
            tok_rows, cot_rows, gate_col, glu_w, lin_w, down_w)
        glu_blocks = glu_bf.reshape(slot_total, N_TP, block_width).transpose(1, 0, 2)
        lin_blocks = lin_bf.reshape(slot_total, N_TP, block_width).transpose(1, 0, 2)
        glu_wblocks = glu_w.reshape(D, N_TP, block_width).transpose(1, 0, 2)
        lin_wblocks = lin_w.reshape(D, N_TP, block_width).transpose(1, 0, 2)

        def add_block(total, pieces):
            glu_piece, lin_piece, glu_wpiece, lin_wpiece = pieces
            term = jnp.dot(glu_piece, glu_wpiece.T, preferred_element_type=jnp.float32)
            term = term + jnp.dot(lin_piece, lin_wpiece.T, preferred_element_type=jnp.float32)
            rounded = lax.optimization_barrier(term.astype(jnp.bfloat16))
            return total + rounded.astype(jnp.float32), None

        total, unused = lax.scan(add_block, jnp.zeros((slot_total, D), jnp.float32),
                                 (glu_blocks, lin_blocks, glu_wblocks, lin_wblocks))
        return total.astype(jnp.bfloat16), gate_part, glu_wgrad, lin_wgrad, down_wgrad

    slot_grads, gate_slots, glu_wgrad, lin_wgrad, down_wgrad = lax.map(
        one_expert, (slot_token, slot_pair, w_glu, w_lin, w_down))
    pair_grads = slot_grads.reshape(-1, D)[slot_index].astype(jnp.float32)
    d_tokens = jnp.sum(pair_grads.reshape(TOKENS, TOP, D), axis=1).astype(jnp.bfloat16)
    d_gates = gate_slots.reshape(-1)[slot_index].reshape(TOKENS, TOP)
    glu_norms = jnp.sum(glu_wgrad * glu_wgrad, axis=2)
    lin_norms = jnp.sum(lin_wgrad * lin_wgrad, axis=2)
    down_norms = jnp.sum(down_wgrad * down_wgrad, axis=2)
    return (d_tokens, d_gates, glu_wgrad, lin_wgrad, down_wgrad, glu_norms, lin_norms, down_norms)
```

```python
import functools

import jax
import jax.numpy as jnp
from jax import lax
from jax.experimental import pallas as pl
from jax.experimental.pallas import tpu as pltpu
from jax.sharding import Mesh
from jax.sharding import PartitionSpec as P

clamp_limit = 7.0
sigmoid_scale = 1.702
HALF = 12
ROWS = 24
f32 = jnp.float32
bf16 = jnp.bfloat16

VMEM = pl.BlockSpec(memory_space=pltpu.VMEM)
SMEM = pl.BlockSpec(memory_space=pltpu.SMEM)


def nt(a, b):
    return lax.dot_general(a, b, (((1,), (1,)), ((), ())), preferred_element_type=f32)


def tn(a, b):
    return lax.dot_general(a, b, (((0,), (0,)), ((), ())), preferred_element_type=f32)


def iota(shape, dim):
    return lax.broadcasted_iota(jnp.int32, shape, dim)


def slot_keys(routes, experts):
    tok = routes.shape[1]
    e = iota((experts, tok), 0)
    first = jnp.broadcast_to(routes[0:1, :], (experts, tok)) == e
    second = jnp.broadcast_to(routes[1:2, :], (experts, tok)) == e
    named = jnp.where(first | second, 1.0, 0.0)
    before = jnp.where(iota((tok, tok), 0) < iota((tok, tok), 1), 1.0, 0.0).astype(bf16)
    rank = jnp.dot(named.astype(bf16), before, preferred_element_type=f32)
    return jnp.where(named > 0.0, rank, -1.0), first


def slot_target(tok, first_slot):
    r = iota((ROWS, 2 * tok), 0)
    h = jnp.where(iota((ROWS, 2 * tok), 1) >= tok, 1, 0)
    mine = jnp.where(r >= HALF, 1, 0) == h
    return jnp.where(mine, (first_slot + r - HALF * h).astype(f32), -2.0)


def pack_kernel(core_ref, routes_ref, gates_ref, tok_ref, cot_ref, out_ref, pick_ref, scale_ref):
    experts = out_ref.shape[0] // ROWS
    tok, width = tok_ref.shape
    key, first = slot_keys(routes_ref[...], experts)
    gate = jnp.where(
        first,
        jnp.broadcast_to(gates_ref[0:1, :], key.shape),
        jnp.broadcast_to(gates_ref[1:2, :], key.shape),
    )
    key2 = jnp.concatenate([key, key], axis=1)
    gate2 = jnp.concatenate([jnp.ones_like(gate), gate], axis=1)
    target = slot_target(tok, core_ref[0] * HALF)
    picks = jnp.concatenate(
        [jnp.where(target == key2[e : e + 1, :], 1.0, 0.0) for e in range(experts)], axis=0
    )
    scales = jnp.concatenate(
        [jnp.broadcast_to(gate2[e : e + 1, :], (ROWS, 2 * tok)) for e in range(experts)], axis=0
    )
    scale_ref[...] = jnp.broadcast_to(
        jnp.sum(picks * scales, axis=1, keepdims=True), scale_ref.shape
    )
    pick_ref[...] = picks.astype(bf16)
    step = min(512, width)

    @pl.loop(0, width // step)
    def _(n):
        cols = pl.ds(pl.multiple_of(n * step, step), step)
        both = jnp.concatenate([tok_ref[:, cols], cot_ref[:, cols]], axis=0)
        rows = jnp.dot(pick_ref[...], both, preferred_element_type=f32)
        scale = jnp.concatenate([scale_ref[...]] * (step // 128), axis=1)
        out_ref[:, cols] = (rows * scale).astype(bf16)


def pack_rows(core, routes, gates, tokens, cotangent, experts):
    tok, width = tokens.shape
    return pl.pallas_call(
        pack_kernel,
        out_shape=jax.ShapeDtypeStruct((experts * ROWS, width), bf16),
        in_specs=[SMEM, VMEM, VMEM, VMEM, VMEM],
        out_specs=VMEM,
        scratch_shapes=[
            pltpu.VMEM((experts * ROWS, 2 * tok), bf16),
            pltpu.VMEM((experts * ROWS, 128), f32),
        ],
        name="pack_rows",
    )(core, routes, gates, tokens, cotangent)


def unit_kernel(rows_ref, wall_ref, wret_ref, grads_ref, msg_ref):
    count = rows_ref.shape[0]
    sources = count // ROWS
    units = wall_ref.shape[0] // 3
    pre = nt(rows_ref[...], wall_ref[...])
    glu_pre = pre[:, :units]
    lin_pre = pre[:, units : 2 * units]
    hid_grad = jnp.roll(pre[:, 2 * units :], -HALF, axis=0)
    keep = lax.rem(iota((count, units), 0), ROWS) < HALF
    glu_clip = jnp.minimum(glu_pre, clamp_limit)
    lin_clip = jnp.clip(lin_pre, -clamp_limit, clamp_limit)
    sig = jax.nn.sigmoid(sigmoid_scale * glu_clip)
    glu_act = glu_clip * sig
    hidden = glu_act * (lin_clip + 1.0)
    slope = sig + sigmoid_scale * glu_clip * sig * (1.0 - sig)
    glu_grad = jnp.where(
        keep & (glu_pre < clamp_limit), hid_grad * (lin_clip + 1.0) * slope, 0.0
    )
    lin_grad = jnp.where(keep & (jnp.abs(lin_pre) < clamp_limit), hid_grad * glu_act, 0.0)
    hidden = jnp.where(keep, hidden, 0.0)
    gate_part = jnp.sum(hid_grad * hidden, axis=1, keepdims=True)
    both = jnp.concatenate([glu_grad, lin_grad], axis=1)
    down = jnp.roll(hidden, HALF, axis=0)
    grads_ref[...] = jnp.concatenate([both, down], axis=1).astype(bf16)
    shifted = jnp.roll(both, HALF, axis=0)
    left = jnp.concatenate([both, shifted], axis=1).astype(bf16)
    lanes = iota((count, 128), 1) == lax.rem(iota((count, 128), 0), ROWS)
    spread = jnp.where(lanes, gate_part, 0.0).reshape(sources, ROWS, 128)
    parts = jnp.sum(spread, axis=1, keepdims=True)
    high = parts.astype(bf16).astype(f32)
    row = iota((sources, 8, 128), 1)
    tail = jnp.where(row == 0, high, jnp.where(row == 1, parts - high, 0.0)).astype(bf16)
    blocks = wret_ref.shape[2] // 128
    for core in range(2):
        part = jnp.dot(left, wret_ref[core], preferred_element_type=f32).astype(bf16)
        for q in range(blocks):
            msg_ref[:, core, q * ROWS : (q + 1) * ROWS, :] = part[
                :, q * 128 : (q + 1) * 128
            ].reshape(sources, ROWS, 128)
        msg_ref[:, core, blocks * ROWS :, :] = tail


def units(rows, wall, wret):
    count = rows.shape[0]
    height = wret.shape[2] // 128 * ROWS + 8
    return pl.pallas_call(
        unit_kernel,
        out_shape=(
            jax.ShapeDtypeStruct((count, wall.shape[0]), bf16),
            jax.ShapeDtypeStruct((count // ROWS, 2, height, 128), bf16),
        ),
        in_specs=[VMEM, VMEM, VMEM],
        out_specs=(VMEM, VMEM),
        name="units",
    )(rows, wall, wret)


def wgrad_kernel(grads_ref, rows_ref, own_ref, other_ref):
    step = min(512, rows_ref.shape[1])

    @pl.loop(0, rows_ref.shape[1] // step)
    def _(n):
        cols = pl.ds(pl.multiple_of(n * step, step), step)
        part = tn(grads_ref[...], rows_ref[:, cols])
        for k in range(3):
            own_ref[k, :, cols] = part[64 * k : 64 * k + 32, :]
            other_ref[k, :, cols] = part[64 * k + 32 : 64 * k + 64, :]


def wgrads(grads, rows):
    shape = jax.ShapeDtypeStruct((3, 32, rows.shape[1]), f32)
    return pl.pallas_call(
        wgrad_kernel,
        out_shape=(shape, shape),
        in_specs=[VMEM, VMEM],
        out_specs=(VMEM, VMEM),
        name="wgrads",
    )(grads, rows)


def total_kernel(own_ref, got_ref, glu_ref, lin_ref, down_ref, norms_ref, down_norms_ref):
    glu = own_ref[0] + got_ref[0]
    lin = own_ref[1] + got_ref[1]
    down = own_ref[2] + got_ref[2]
    glu_ref[...] = glu
    lin_ref[...] = lin
    down_ref[...] = down
    norms_ref[0:1, :] = jnp.sum(glu * glu, axis=0, keepdims=True)
    norms_ref[1:2, :] = jnp.sum(lin * lin, axis=0, keepdims=True)
    each = jnp.sum(down * down, axis=1, keepdims=True)
    spread = jnp.where(iota((32, 128), 0) == iota((32, 128), 1), each, 0.0)
    down_norms_ref[...] = jnp.sum(spread, axis=0, keepdims=True)


def totals(own, got):
    width = own.shape[2]
    shape = jax.ShapeDtypeStruct((32, width), f32)
    return pl.pallas_call(
        total_kernel,
        out_shape=(
            shape,
            shape,
            shape,
            jax.ShapeDtypeStruct((2, width), f32),
            jax.ShapeDtypeStruct((1, 128), f32),
        ),
        in_specs=[VMEM, VMEM],
        out_specs=(VMEM,) * 5,
        name="totals",
    )(own, got)


def combine_kernel(routes_ref, back_ref, norms_ref, got_ref, msg_ref):
    experts = back_ref.shape[0]
    height = back_ref.shape[2]
    blocks = (height - 8) // ROWS
    tok = routes_ref.shape[1]
    depth = msg_ref.shape[0]
    key, first = slot_keys(routes_ref[...], experts)
    key2 = jnp.concatenate([key, key], axis=1)
    targets = [slot_target(tok, core * HALF) for core in range(2)]
    picks = jnp.concatenate(
        [
            jnp.where(targets[core] == key2[e : e + 1, :], 1.0, 0.0)
            for e in range(experts)
            for core in range(2)
        ],
        axis=0,
    )
    pick = picks.astype(bf16)
    for q in range(blocks):
        rows = back_ref[:, :, q * ROWS : (q + 1) * ROWS, :].reshape(experts * 2 * ROWS, 128)
        sums = tn(rows, pick).astype(bf16)
        for h in range(2):
            for b in range(2):
                msg_ref[h * (depth // 2) + 2 * q + b, 0:64, :] = sums[
                    64 * b : 64 * b + 64, h * tok : (h + 1) * tok
                ]
    tail = back_ref[:, :, blocks * ROWS :, :].astype(f32).reshape(experts * 2, 8, 128)
    parts = tail[:, 0:1, :] + tail[:, 1:2, :]
    spread = jnp.broadcast_to(parts, (experts * 2, ROWS, 128)).reshape(experts * 2 * ROWS, 128)
    shape = spread.shape
    lanes = iota(shape, 1) == lax.rem(iota(shape, 0), ROWS)
    column = jnp.sum(jnp.where(lanes, spread, 0.0), axis=1, keepdims=True)
    placed = (picks[:, :tok] * column).reshape(experts, 2 * ROWS, tok)
    each = jnp.sum(placed, axis=1)
    named_first = jnp.sum(jnp.where(first, each, 0.0), axis=0, keepdims=True)
    named_second = jnp.sum(jnp.where(first, 0.0, each), axis=0, keepdims=True)
    high_first = named_first.astype(bf16).astype(f32)
    high_second = named_second.astype(bf16).astype(f32)
    row = iota((8, 128), 0)
    gate_rows = jnp.where(row == 0, high_first, jnp.where(row == 1, high_second, 0.0))
    gate_rows = jnp.where(row == 2, named_first - high_first, gate_rows)
    gate_rows = jnp.where(row == 3, named_second - high_second, gate_rows)
    normed = norms_ref[...] + got_ref[...]
    count = normed.shape[1] // 128
    lines = jnp.concatenate(
        [normed[k : k + 1, n * 128 : (n + 1) * 128] for k in range(2) for n in range(count)], axis=0
    )
    extra = jnp.concatenate([lines, gate_rows], axis=0).astype(bf16)
    for z in range(depth):
        msg_ref[z, 64:, :] = extra


def combine(routes, back, norms, got, depth):
    height = 64 + 2 * norms.shape[1] // 128 + 8
    return pl.pallas_call(
        combine_kernel,
        out_shape=jax.ShapeDtypeStruct((depth, height, 128), bf16),
        in_specs=[VMEM] * 4,
        out_specs=VMEM,
        name="combine",
    )(routes, back, norms, got)


def finish_kernel(parts_ref, gates_ref, tok_ref, gate_ref, norms_ref):
    total = jnp.sum(parts_ref[...].astype(f32), axis=0)
    lines = norms_ref.shape[0]
    tok_ref[...] = total[:64, :].astype(bf16)
    norms_ref[...] = total[64 : 64 + lines, :]
    tail = total[64 + lines :, :]
    gate_ref[...] = (tail[0:2, :] + tail[2:4, :]) / gates_ref[...]


def finish(parts, gates):
    lines = parts.shape[1] - 72
    return pl.pallas_call(
        finish_kernel,
        out_shape=(
            jax.ShapeDtypeStruct((64, 128), bf16),
            jax.ShapeDtypeStruct((2, 128), f32),
            jax.ShapeDtypeStruct((lines, 128), f32),
        ),
        in_specs=[VMEM] * 2,
        out_specs=(VMEM,) * 3,
        name="finish",
    )(parts, gates)


def swap(x):
    return lax.ppermute(x, "tp_1", [(0, 1), (1, 0)])


def shards(tokens, routes, gates, cotangent, w_glu, w_lin, w_down):
    experts = lax.axis_size("ep")
    depth = lax.axis_size("tp_0")
    tok, width = tokens.shape
    core = lax.axis_index("tp_1").astype(jnp.int32).reshape(1)
    routes_t, gates_t = routes.T, gates.T
    glu_t, lin_t, down = w_glu[0].T, w_lin[0].T, w_down[0]

    packed = pack_rows(core, routes_t, gates_t, tokens, cotangent, experts)
    rows = lax.all_to_all(packed.reshape(experts, ROWS, width), "ep", 0, 0, tiled=True)
    rows = rows.reshape(experts * ROWS, width)

    glu_o, lin_o, down_o = swap(glu_t), swap(lin_t), swap(down)
    wall = jnp.concatenate([glu_t, glu_o, lin_t, lin_o, down, down_o], axis=0)
    inner = wall[:128].reshape(128, 2, depth // 2, 2, 64)
    wret = inner.transpose(3, 1, 0, 2, 4).reshape(2, 256, width // 4)

    grads, msg = units(rows, wall, wret)
    msg = msg.reshape(experts * 2, *msg.shape[2:])
    back = lax.all_to_all(msg, ("ep", "tp_1"), 0, 0, tiled=True)
    back = back.reshape(experts, 2, *msg.shape[1:])

    own, other = wgrads(grads, rows)
    glu_wg, lin_wg, down_wg, norms, down_norms = totals(own, swap(other))
    msg = combine(routes_t, back, norms, swap(norms), depth)
    parts = lax.all_to_all(msg, "tp_0", 0, 0, tiled=True)
    tok_t, gate_t, lines = finish(parts, gates_t)
    lines = lines.reshape(2, width)
    return (
        tok_t.T,
        gate_t.T,
        glu_wg.T[None],
        lin_wg.T[None],
        down_wg[None],
        lines[0:1],
        lines[1:2],
        down_norms[:, :32],
    )


def solution(mesh):
    depth = mesh.shape["tp"] // 2
    split = Mesh(mesh.devices.reshape(mesh.shape["ep"], depth, 2), ("ep", "tp_0", "tp_1"))
    tp = ("tp_0", "tp_1")
    return jax.shard_map(
        shards,
        mesh=split,
        in_specs=(
            P("ep", None),
            P("ep", None),
            P("ep", None),
            P("ep", None),
            P("ep", None, tp),
            P("ep", None, tp),
            P("ep", tp, None),
        ),
        out_specs=(
            P("ep", tp),
            P("ep", None),
            P("ep", None, tp),
            P("ep", None, tp),
            P("ep", tp, None),
            P("ep", None),
            P("ep", None),
            P("ep", tp),
        ),
        check_vma=False,
    )
```

```python
import functools

import jax
import jax.numpy as jnp
from jax import lax
from jax.experimental import pallas as pl
from jax.experimental.pallas import tpu as pltpu
from jax.sharding import Mesh
from jax.sharding import PartitionSpec as P

clamp_limit = 7.0
sigmoid_scale = 1.702
HALF = 12
LIMIT = 24 * 1024 * 1024
ROWS = 24
f32 = jnp.float32
bf16 = jnp.bfloat16

VMEM = pl.BlockSpec(memory_space=pltpu.VMEM)
SMEM = pl.BlockSpec(memory_space=pltpu.SMEM)


def nt(a, b):
    return lax.dot_general(a, b, (((1,), (1,)), ((), ())), preferred_element_type=f32)


def tn(a, b):
    return lax.dot_general(a, b, (((0,), (0,)), ((), ())), preferred_element_type=f32)


def iota(shape, dim):
    return lax.broadcasted_iota(jnp.int32, shape, dim)


def slot_keys(routes, experts):
    tok = routes.shape[1]
    e = iota((experts, tok), 0)
    first = jnp.broadcast_to(routes[0:1, :], (experts, tok)) == e
    second = jnp.broadcast_to(routes[1:2, :], (experts, tok)) == e
    named = jnp.where(first | second, 1.0, 0.0)
    before = jnp.where(iota((tok, tok), 0) < iota((tok, tok), 1), 1.0, 0.0).astype(bf16)
    rank = jnp.dot(named.astype(bf16), before, preferred_element_type=f32)
    return jnp.where(named > 0.0, rank, -1.0), first


def slot_target(tok, first_slot):
    r = iota((ROWS, 2 * tok), 0)
    h = jnp.where(iota((ROWS, 2 * tok), 1) >= tok, 1, 0)
    mine = jnp.where(r >= HALF, 1, 0) == h
    return jnp.where(mine, (first_slot + r - HALF * h).astype(f32), -2.0)


def pack_kernel(core_ref, routes_ref, gates_ref, tok_ref, cot_ref, out_ref, pick_ref, scale_ref):
    experts = out_ref.shape[0] // ROWS
    tok, width = tok_ref.shape
    key, first = slot_keys(routes_ref[...], experts)
    gate = jnp.where(
        first,
        jnp.broadcast_to(gates_ref[0:1, :], key.shape),
        jnp.broadcast_to(gates_ref[1:2, :], key.shape),
    )
    key2 = jnp.concatenate([key, key], axis=1)
    gate2 = jnp.concatenate([jnp.ones_like(gate), gate], axis=1)
    target = slot_target(tok, core_ref[0] * HALF)
    picks = jnp.concatenate(
        [jnp.where(target == key2[e : e + 1, :], 1.0, 0.0) for e in range(experts)], axis=0
    )
    scales = jnp.concatenate(
        [jnp.broadcast_to(gate2[e : e + 1, :], (ROWS, 2 * tok)) for e in range(experts)], axis=0
    )
    scale_ref[...] = jnp.broadcast_to(
        jnp.sum(picks * scales, axis=1, keepdims=True), scale_ref.shape
    )
    pick_ref[...] = picks.astype(bf16)
    step = min(512, width)

    @pl.loop(0, width // step)
    def _(n):
        cols = pl.ds(pl.multiple_of(n * step, step), step)
        both = jnp.concatenate([tok_ref[:, cols], cot_ref[:, cols]], axis=0)
        rows = jnp.dot(pick_ref[...], both, preferred_element_type=f32)
        scale = jnp.concatenate([scale_ref[...]] * (step // 128), axis=1)
        out_ref[:, cols] = (rows * scale).astype(bf16)


def pack_rows(core, routes, gates, tokens, cotangent, experts):
    tok, width = tokens.shape
    return pl.pallas_call(
        pack_kernel,
        out_shape=jax.ShapeDtypeStruct((experts * ROWS, width), bf16),
        in_specs=[SMEM, VMEM, VMEM, VMEM, VMEM],
        out_specs=VMEM,
        scratch_shapes=[
            pltpu.VMEM((experts * ROWS, 2 * tok), bf16),
            pltpu.VMEM((experts * ROWS, 128), f32),
        ],
        name="pack_rows",
    )(core, routes, gates, tokens, cotangent)


def unit_kernel(rows_ref, wall_ref, wret_ref, grads_ref, msg_ref):
    count = rows_ref.shape[0]
    sources = count // ROWS
    units = wall_ref.shape[0] // 3
    pre = nt(rows_ref[...], wall_ref[...])
    glu_pre = pre[:, :units]
    lin_pre = pre[:, units : 2 * units]
    hid_grad = jnp.roll(pre[:, 2 * units :], -HALF, axis=0)
    keep = lax.rem(iota((count, units), 0), ROWS) < HALF
    glu_clip = jnp.minimum(glu_pre, clamp_limit)
    lin_clip = jnp.clip(lin_pre, -clamp_limit, clamp_limit)
    sig = jax.nn.sigmoid(sigmoid_scale * glu_clip)
    glu_act = glu_clip * sig
    hidden = glu_act * (lin_clip + 1.0)
    slope = sig + sigmoid_scale * glu_clip * sig * (1.0 - sig)
    glu_grad = jnp.where(
        keep & (glu_pre < clamp_limit), hid_grad * (lin_clip + 1.0) * slope, 0.0
    )
    lin_grad = jnp.where(keep & (jnp.abs(lin_pre) < clamp_limit), hid_grad * glu_act, 0.0)
    hidden = jnp.where(keep, hidden, 0.0)
    gate_part = jnp.sum(hid_grad * hidden, axis=1, keepdims=True)
    both = jnp.concatenate([glu_grad, lin_grad], axis=1)
    down = jnp.roll(hidden, HALF, axis=0)
    grads_ref[...] = jnp.concatenate([both, down], axis=1).astype(bf16)
    shifted = jnp.roll(both, HALF, axis=0)
    left = jnp.concatenate([both, shifted], axis=1).astype(bf16)
    lanes = iota((count, 128), 1) == lax.rem(iota((count, 128), 0), ROWS)
    spread = jnp.where(lanes, gate_part, 0.0).reshape(sources, ROWS, 128)
    parts = jnp.sum(spread, axis=1, keepdims=True)
    high = parts.astype(bf16).astype(f32)
    row = iota((sources, 8, 128), 1)
    tail = jnp.where(row == 0, high, jnp.where(row == 1, parts - high, 0.0)).astype(bf16)
    blocks = wret_ref.shape[2] // 128
    for core in range(2):
        part = jnp.dot(left, wret_ref[core], preferred_element_type=f32).astype(bf16)
        for q in range(blocks):
            msg_ref[:, core, q * ROWS : (q + 1) * ROWS, :] = part[
                :, q * 128 : (q + 1) * 128
            ].reshape(sources, ROWS, 128)
        msg_ref[:, core, blocks * ROWS :, :] = tail


def units(rows, wall, wret):
    count = rows.shape[0]
    height = wret.shape[2] // 128 * ROWS + 8
    return pl.pallas_call(
        unit_kernel,
        out_shape=(
            jax.ShapeDtypeStruct((count, wall.shape[0]), bf16),
            jax.ShapeDtypeStruct((count // ROWS, 2, height, 128), bf16),
        ),
        in_specs=[VMEM, VMEM, VMEM],
        out_specs=(VMEM, VMEM),
        compiler_params=pltpu.CompilerParams(vmem_limit_bytes=LIMIT),
        name="units",
    )(rows, wall, wret)


def wgrad_kernel(grads_ref, rows_ref, own_ref, other_ref):
    step = min(512, rows_ref.shape[1])

    @pl.loop(0, rows_ref.shape[1] // step)
    def _(n):
        cols = pl.ds(pl.multiple_of(n * step, step), step)
        part = tn(grads_ref[...], rows_ref[:, cols])
        for k in range(3):
            own_ref[k, :, cols] = part[64 * k : 64 * k + 32, :]
            other_ref[k, :, cols] = part[64 * k + 32 : 64 * k + 64, :]


def wgrads(grads, rows):
    shape = jax.ShapeDtypeStruct((3, 32, rows.shape[1]), f32)
    return pl.pallas_call(
        wgrad_kernel,
        out_shape=(shape, shape),
        in_specs=[VMEM, VMEM],
        out_specs=(VMEM, VMEM),
        compiler_params=pltpu.CompilerParams(vmem_limit_bytes=LIMIT),
        name="wgrads",
    )(grads, rows)


def total_kernel(own_ref, got_ref, glu_ref, lin_ref, down_ref, norms_ref, down_norms_ref):
    glu = own_ref[0] + got_ref[0]
    lin = own_ref[1] + got_ref[1]
    down = own_ref[2] + got_ref[2]
    glu_ref[...] = glu
    lin_ref[...] = lin
    down_ref[...] = down
    norms_ref[0:1, :] = jnp.sum(glu * glu, axis=0, keepdims=True)
    norms_ref[1:2, :] = jnp.sum(lin * lin, axis=0, keepdims=True)
    each = jnp.sum(down * down, axis=1, keepdims=True)
    spread = jnp.where(iota((32, 128), 0) == iota((32, 128), 1), each, 0.0)
    down_norms_ref[...] = jnp.sum(spread, axis=0, keepdims=True)


def totals(own, got):
    width = own.shape[2]
    shape = jax.ShapeDtypeStruct((32, width), f32)
    return pl.pallas_call(
        total_kernel,
        out_shape=(
            shape,
            shape,
            shape,
            jax.ShapeDtypeStruct((2, width), f32),
            jax.ShapeDtypeStruct((1, 128), f32),
        ),
        in_specs=[VMEM, VMEM],
        out_specs=(VMEM,) * 5,
        compiler_params=pltpu.CompilerParams(vmem_limit_bytes=LIMIT),
        name="totals",
    )(own, got)


def combine_kernel(routes_ref, back_ref, norms_ref, got_ref, msg_ref):
    experts = back_ref.shape[0]
    height = back_ref.shape[2]
    blocks = (height - 8) // ROWS
    tok = routes_ref.shape[1]
    depth = msg_ref.shape[0]
    key, first = slot_keys(routes_ref[...], experts)
    key2 = jnp.concatenate([key, key], axis=1)
    targets = [slot_target(tok, core * HALF) for core in range(2)]
    picks = jnp.concatenate(
        [
            jnp.where(targets[core] == key2[e : e + 1, :], 1.0, 0.0)
            for e in range(experts)
            for core in range(2)
        ],
        axis=0,
    )
    pick = picks.astype(bf16)
    for q in range(blocks):
        rows = back_ref[:, :, q * ROWS : (q + 1) * ROWS, :].reshape(experts * 2 * ROWS, 128)
        sums = tn(rows, pick).astype(bf16)
        for h in range(2):
            for b in range(2):
                msg_ref[h * (depth // 2) + 2 * q + b, 0:64, :] = sums[
                    64 * b : 64 * b + 64, h * tok : (h + 1) * tok
                ]
    tail = back_ref[:, :, blocks * ROWS :, :].astype(f32).reshape(experts * 2, 8, 128)
    parts = tail[:, 0:1, :] + tail[:, 1:2, :]
    spread = jnp.broadcast_to(parts, (experts * 2, ROWS, 128)).reshape(experts * 2 * ROWS, 128)
    shape = spread.shape
    lanes = iota(shape, 1) == lax.rem(iota(shape, 0), ROWS)
    column = jnp.sum(jnp.where(lanes, spread, 0.0), axis=1, keepdims=True)
    placed = (picks[:, :tok] * column).reshape(experts, 2 * ROWS, tok)
    each = jnp.sum(placed, axis=1)
    named_first = jnp.sum(jnp.where(first, each, 0.0), axis=0, keepdims=True)
    named_second = jnp.sum(jnp.where(first, 0.0, each), axis=0, keepdims=True)
    high_first = named_first.astype(bf16).astype(f32)
    high_second = named_second.astype(bf16).astype(f32)
    row = iota((8, 128), 0)
    gate_rows = jnp.where(row == 0, high_first, jnp.where(row == 1, high_second, 0.0))
    gate_rows = jnp.where(row == 2, named_first - high_first, gate_rows)
    gate_rows = jnp.where(row == 3, named_second - high_second, gate_rows)
    normed = norms_ref[...] + got_ref[...]
    count = normed.shape[1] // 128
    lines = jnp.concatenate(
        [normed[k : k + 1, n * 128 : (n + 1) * 128] for k in range(2) for n in range(count)], axis=0
    )
    extra = jnp.concatenate([lines, gate_rows], axis=0).astype(bf16)
    for z in range(depth):
        msg_ref[z, 64:, :] = extra


def combine(routes, back, norms, got, depth):
    height = 64 + 2 * norms.shape[1] // 128 + 8
    return pl.pallas_call(
        combine_kernel,
        out_shape=jax.ShapeDtypeStruct((depth, height, 128), bf16),
        in_specs=[VMEM] * 4,
        out_specs=VMEM,
        compiler_params=pltpu.CompilerParams(vmem_limit_bytes=LIMIT),
        name="combine",
    )(routes, back, norms, got)


def finish_kernel(parts_ref, gates_ref, tok_ref, gate_ref, glu_ref, lin_ref):
    total = jnp.sum(parts_ref[...].astype(f32), axis=0)
    lines = glu_ref.shape[0]
    tok_ref[...] = total[:64, :].astype(bf16)
    glu_ref[...] = total[64 : 64 + lines, :]
    lin_ref[...] = total[64 + lines : 64 + 2 * lines, :]
    tail = total[64 + 2 * lines :, :]
    gate_ref[...] = (tail[0:2, :] + tail[2:4, :]) / gates_ref[...]


def finish(parts, gates):
    lines = (parts.shape[1] - 72) // 2
    return pl.pallas_call(
        finish_kernel,
        out_shape=(
            jax.ShapeDtypeStruct((64, 128), bf16),
            jax.ShapeDtypeStruct((2, 128), f32),
            jax.ShapeDtypeStruct((lines, 128), f32),
            jax.ShapeDtypeStruct((lines, 128), f32),
        ),
        in_specs=[VMEM] * 2,
        out_specs=(VMEM,) * 4,
        compiler_params=pltpu.CompilerParams(vmem_limit_bytes=LIMIT),
        name="finish",
    )(parts, gates)


def swap(x):
    return lax.ppermute(x, "tp_1", [(0, 1), (1, 0)])


def shards(tokens, routes, gates, cotangent, w_glu, w_lin, w_down):
    experts = lax.axis_size("ep")
    depth = lax.axis_size("tp_0")
    tok, width = tokens.shape
    core = lax.axis_index("tp_1").astype(jnp.int32).reshape(1)
    routes_t, gates_t = routes.T, gates.T
    glu_t, lin_t, down = w_glu[0].T, w_lin[0].T, w_down[0]

    packed = pack_rows(core, routes_t, gates_t, tokens, cotangent, experts)
    rows = lax.all_to_all(packed.reshape(experts, ROWS, width), "ep", 0, 0, tiled=True)
    rows = rows.reshape(experts * ROWS, width)

    glu_o, lin_o, down_o = swap(glu_t), swap(lin_t), swap(down)
    wall = jnp.concatenate([glu_t, glu_o, lin_t, lin_o, down, down_o], axis=0)
    inner = wall[:128].reshape(128, 2, depth // 2, 2, 64)
    wret = inner.transpose(3, 1, 0, 2, 4).reshape(2, 256, width // 4)

    grads, msg = units(rows, wall, wret)
    msg = msg.reshape(experts * 2, *msg.shape[2:])
    back = lax.all_to_all(msg, ("ep", "tp_1"), 0, 0, tiled=True)
    back = back.reshape(experts, 2, *msg.shape[1:])

    own, other = wgrads(grads, rows)
    glu_wg, lin_wg, down_wg, norms, down_norms = totals(own, swap(other))
    msg = combine(routes_t, back, norms, swap(norms), depth)
    parts = lax.all_to_all(msg, "tp_0", 0, 0, tiled=True)
    tok_t, gate_t, glu_norms, lin_norms = finish(parts, gates_t)
    return (
        tok_t.T,
        gate_t.T,
        glu_wg.T[None],
        lin_wg.T[None],
        down_wg[None],
        glu_norms.reshape(1, width),
        lin_norms.reshape(1, width),
        down_norms[:, :32],
    )


def solution(mesh):
    depth = mesh.shape["tp"] // 2
    split = Mesh(mesh.devices.reshape(mesh.shape["ep"], depth, 2), ("ep", "tp_0", "tp_1"))
    tp = ("tp_0", "tp_1")
    return jax.shard_map(
        shards,
        mesh=split,
        in_specs=(
            P("ep", None),
            P("ep", None),
            P("ep", None),
            P("ep", None),
            P("ep", None, tp),
            P("ep", None, tp),
            P("ep", tp, None),
        ),
        out_specs=(
            P("ep", tp),
            P("ep", None),
            P("ep", None, tp),
            P("ep", None, tp),
            P("ep", tp, None),
            P("ep", None),
            P("ep", None),
            P("ep", tp),
        ),
        check_vma=False,
    )
```

```python
import jax
import jax.numpy as jnp
from jax import lax
from jax.experimental import pallas as pl
from jax.experimental.pallas import tpu as pltpu
from jax.sharding import Mesh
from jax.sharding import PartitionSpec as P

clamp_limit = 7.0
sigmoid_scale = 1.702
HALF = 12
LIMIT = 24 * 1024 * 1024
ROWS = 24
f32 = jnp.float32
bf16 = jnp.bfloat16

VMEM = pl.BlockSpec(memory_space=pltpu.VMEM)
SMEM = pl.BlockSpec(memory_space=pltpu.SMEM)


def nt(a, b):
    return lax.dot_general(a, b, (((1,), (1,)), ((), ())), preferred_element_type=f32)


def tn(a, b):
    return lax.dot_general(a, b, (((0,), (0,)), ((), ())), preferred_element_type=f32)


def iota(shape, dim):
    return lax.broadcasted_iota(jnp.int32, shape, dim)


def block(j, side):
    return pl.ds(pl.multiple_of((2 * j + side) * 128, 128), 128)


def slot_keys(routes, experts):
    tok = routes.shape[1]
    e = iota((experts, tok), 0)
    first = jnp.broadcast_to(routes[0:1, :], (experts, tok)) == e
    second = jnp.broadcast_to(routes[1:2, :], (experts, tok)) == e
    named = jnp.where(first | second, 1.0, 0.0)
    before = jnp.where(iota((tok, tok), 0) < iota((tok, tok), 1), 1.0, 0.0).astype(bf16)
    rank = jnp.dot(named.astype(bf16), before, preferred_element_type=f32)
    return jnp.where(named > 0.0, rank, -1.0), first


def slot_target(tok, first_slot):
    r = iota((ROWS, 2 * tok), 0)
    h = jnp.where(iota((ROWS, 2 * tok), 1) >= tok, 1, 0)
    mine = jnp.where(r >= HALF, 1, 0) == h
    return jnp.where(mine, (first_slot + r - HALF * h).astype(f32), -2.0)


def pack_kernel(place_ref, core_ref, routes_ref, gates_ref, tok_ref, cot_ref, out_ref, pick_ref, scale_ref):
    experts = out_ref.shape[0] // ROWS
    tok = tok_ref.shape[0]
    width = out_ref.shape[1]
    side = place_ref[0]
    key, first = slot_keys(routes_ref[...], experts)
    gate = jnp.where(
        first,
        jnp.broadcast_to(gates_ref[0:1, :], key.shape),
        jnp.broadcast_to(gates_ref[1:2, :], key.shape),
    )
    key2 = jnp.concatenate([key, key], axis=1)
    gate2 = jnp.concatenate([jnp.ones_like(gate), gate], axis=1)
    target = slot_target(tok, core_ref[0] * HALF)
    picks = jnp.concatenate(
        [jnp.where(target == key2[e : e + 1, :], 1.0, 0.0) for e in range(experts)], axis=0
    )
    scales = jnp.concatenate(
        [jnp.broadcast_to(gate2[e : e + 1, :], (ROWS, 2 * tok)) for e in range(experts)], axis=0
    )
    scale_ref[...] = jnp.broadcast_to(
        jnp.sum(picks * scales, axis=1, keepdims=True), scale_ref.shape
    )
    pick_ref[...] = picks.astype(bf16)
    wide = min(4, width // 128)

    @pl.loop(0, width // (128 * wide))
    def _(n):
        both = jnp.concatenate(
            [
                jnp.concatenate([ref[:, block(n * wide + k, side)] for k in range(wide)], axis=1)
                for ref in (tok_ref, cot_ref)
            ],
            axis=0,
        )
        rows = jnp.dot(pick_ref[...], both, preferred_element_type=f32)
        scale = jnp.concatenate([scale_ref[...]] * wide, axis=1)
        cols = pl.ds(pl.multiple_of(n * 128 * wide, 128 * wide), 128 * wide)
        out_ref[:, cols] = (rows * scale).astype(bf16)


def pack_rows(place, core, routes, gates, tokens, cotangent, experts):
    tok, width = tokens.shape
    return pl.pallas_call(
        pack_kernel,
        out_shape=jax.ShapeDtypeStruct((experts * ROWS, width // 2), bf16),
        in_specs=[SMEM, SMEM, VMEM, VMEM, VMEM, VMEM],
        out_specs=VMEM,
        scratch_shapes=[
            pltpu.VMEM((experts * ROWS, 2 * tok), bf16),
            pltpu.VMEM((experts * ROWS, 128), f32),
        ],
        name="pack_rows",
    )(place, core, routes, gates, tokens, cotangent)


def part_kernel(place_ref, glu_ref, lin_ref, down_ref, keep_ref, send_ref):
    side = place_ref[0]
    for k, ref in enumerate((glu_ref, lin_ref, down_ref)):
        for j in range(keep_ref.shape[1] // 128):
            cols = slice(128 * j, 128 * j + 128)
            keep_ref[32 * k : 32 * k + 32, cols] = ref[:, block(j, side)]
            send_ref[32 * k : 32 * k + 32, cols] = ref[:, block(j, 1 - side)]


def part_weights(place, glu, lin, down):
    shape = jax.ShapeDtypeStruct((96, glu.shape[1] // 2), bf16)
    return pl.pallas_call(
        part_kernel,
        out_shape=(shape, shape),
        in_specs=[SMEM, VMEM, VMEM, VMEM],
        out_specs=(VMEM,) * 2,
        compiler_params=pltpu.CompilerParams(vmem_limit_bytes=LIMIT),
        name="part_weights",
    )(place, glu, lin, down)


def gather_kernel(place_ref, keep_ref, side_ref, core_ref, cross_ref, wall_ref, wret_ref):
    def fill(order):
        for k in range(3):
            for n, ref in enumerate(order):
                at = 128 * k + 32 * n
                wall_ref[at : at + 32, :] = ref[32 * k : 32 * k + 32, :]

    @pl.when(place_ref[0] == 0)
    def _():
        fill((keep_ref, side_ref, core_ref, cross_ref))

    @pl.when(place_ref[0] == 1)
    def _():
        fill((side_ref, keep_ref, cross_ref, core_ref))

    half = wall_ref.shape[1] // 2
    low = iota((256, 128), 1) < 64
    for h in range(2):
        for q in range(half // 256):
            at = h * half + q * 256
            one = wall_ref[0:256, at : at + 128].astype(f32)
            two = wall_ref[0:256, at + 128 : at + 256].astype(f32)
            even = jnp.where(low, one, pltpu.roll(two, 64, 1))
            odd = jnp.where(low, pltpu.roll(one, 64, 1), two)
            cols = slice(128 * q, 128 * q + 128)
            wret_ref[0, 256 * h : 256 * h + 256, cols] = even.astype(bf16)
            wret_ref[1, 256 * h : 256 * h + 256, cols] = odd.astype(bf16)


def gather_weights(place, keep, side, core, cross):
    width = keep.shape[1]
    return pl.pallas_call(
        gather_kernel,
        out_shape=(
            jax.ShapeDtypeStruct((384, width), bf16),
            jax.ShapeDtypeStruct((2, 512, width // 4), bf16),
        ),
        in_specs=[SMEM] + [VMEM] * 4,
        out_specs=(VMEM,) * 2,
        compiler_params=pltpu.CompilerParams(vmem_limit_bytes=LIMIT),
        name="gather_weights",
    )(place, keep, side, core, cross)


def pre_kernel(rows_ref, wall_ref, out_ref):
    count = rows_ref.shape[0]
    pre = nt(rows_ref[...], wall_ref[...])
    upper = lax.rem(iota((count, 128), 0), ROWS) < HALF
    out_ref[0:count, :] = jnp.where(upper, pre[:, :128], pre[:, 256:])
    lin = pre[:, 128:256].reshape(count // (2 * ROWS), 2, ROWS, 128)
    moved = jnp.roll(pre[:, 128:256], HALF, axis=0).reshape(lin.shape)
    top = iota((count // (2 * ROWS), ROWS, 128), 1) < HALF
    out_ref[count:, :] = jnp.where(top, lin[:, 0], moved[:, 1]).reshape(count // 2, 128)


def pre_parts(rows, wall):
    count = rows.shape[0]
    return pl.pallas_call(
        pre_kernel,
        out_shape=jax.ShapeDtypeStruct((count + count // 2, 128), f32),
        in_specs=[VMEM, VMEM],
        out_specs=VMEM,
        compiler_params=pltpu.CompilerParams(vmem_limit_bytes=LIMIT),
        name="pre_parts",
    )(rows, wall)


def unit_kernel(mine_ref, got_ref, wret_ref, grads_ref, msg_ref):
    count = grads_ref.shape[0]
    sources = count // ROWS
    units = 128
    glu_pre = mine_ref[0:count, :] + got_ref[0:count, :]
    hid_grad = jnp.roll(glu_pre, -HALF, axis=0)
    lin = mine_ref[count:, :] + got_ref[count:, :]
    moved = jnp.roll(lin, -HALF, axis=0)
    lin_pre = jnp.concatenate(
        [lin.reshape(sources // 2, 1, ROWS, units), moved.reshape(sources // 2, 1, ROWS, units)],
        axis=1,
    ).reshape(count, units)
    keep = lax.rem(iota((count, units), 0), ROWS) < HALF
    glu_clip = jnp.minimum(glu_pre, clamp_limit)
    lin_clip = jnp.clip(lin_pre, -clamp_limit, clamp_limit)
    sig = jax.nn.sigmoid(sigmoid_scale * glu_clip)
    glu_act = glu_clip * sig
    hidden = glu_act * (lin_clip + 1.0)
    slope = sig + sigmoid_scale * glu_clip * sig * (1.0 - sig)
    glu_grad = jnp.where(
        keep & (glu_pre < clamp_limit), hid_grad * (lin_clip + 1.0) * slope, 0.0
    )
    lin_grad = jnp.where(keep & (jnp.abs(lin_pre) < clamp_limit), hid_grad * glu_act, 0.0)
    hidden = jnp.where(keep, hidden, 0.0)
    gate_part = jnp.sum(hid_grad * hidden, axis=1, keepdims=True)
    both = jnp.concatenate([glu_grad, lin_grad], axis=1)
    down = jnp.roll(hidden, HALF, axis=0)
    grads_ref[...] = jnp.concatenate([both, down], axis=1).astype(bf16)
    shifted = jnp.roll(both, HALF, axis=0)
    left = jnp.concatenate([both, shifted], axis=1).astype(bf16)
    lanes = iota((count, 128), 1) == lax.rem(iota((count, 128), 0), ROWS)
    spread = jnp.where(lanes, gate_part, 0.0).reshape(sources, ROWS, 128)
    parts = jnp.sum(spread, axis=1, keepdims=True)
    high = parts.astype(bf16).astype(f32)
    row = iota((sources, 8, 128), 1)
    tail = jnp.where(row == 0, high, jnp.where(row == 1, parts - high, 0.0)).astype(bf16)
    blocks = wret_ref.shape[2] // 128
    for core in range(2):
        part = jnp.dot(left, wret_ref[core], preferred_element_type=f32).astype(bf16)
        for q in range(blocks):
            msg_ref[:, core, q * ROWS : (q + 1) * ROWS, :] = part[
                :, q * 128 : (q + 1) * 128
            ].reshape(sources, ROWS, 128)
        msg_ref[:, core, blocks * ROWS :, :] = tail


def units(mine, got, wret):
    count = mine.shape[0] // 3 * 2
    height = wret.shape[2] // 128 * ROWS + 8
    return pl.pallas_call(
        unit_kernel,
        out_shape=(
            jax.ShapeDtypeStruct((count, 384), bf16),
            jax.ShapeDtypeStruct((count // ROWS, 2, height, 128), bf16),
        ),
        in_specs=[VMEM, VMEM, VMEM],
        out_specs=(VMEM, VMEM),
        compiler_params=pltpu.CompilerParams(vmem_limit_bytes=LIMIT),
        name="units",
    )(mine, got, wret)


def wgrad_kernel(grads_ref, rows_ref, part_ref, down_ref):
    step = min(512, rows_ref.shape[1])

    @pl.loop(0, rows_ref.shape[1] // step)
    def _(n):
        cols = pl.ds(pl.multiple_of(n * step, step), step)
        part = tn(grads_ref[...], rows_ref[:, cols])
        for k in range(4):
            part_ref[k, :, cols] = part[64 * k : 64 * k + 64, :]
        down_ref[:, cols] = part[256:320, :]
        part_ref[4, :, cols] = part[320:384, :]


def wgrads(grads, rows):
    width = rows.shape[1]
    return pl.pallas_call(
        wgrad_kernel,
        out_shape=(
            jax.ShapeDtypeStruct((5, 64, width), f32),
            jax.ShapeDtypeStruct((64, width), f32),
        ),
        in_specs=[VMEM, VMEM],
        out_specs=(VMEM,) * 2,
        compiler_params=pltpu.CompilerParams(vmem_limit_bytes=LIMIT),
        name="wgrads",
    )(grads, rows)


def total_kernel(place_ref, own_ref, down_ref, got_ref, keep_ref, send_ref, norms_ref):
    side = place_ref[0]
    for k in range(3):
        if k < 2:
            mine = own_ref[2 * k] + got_ref[2 * k + 1]
            other = own_ref[2 * k + 1] + got_ref[2 * k]
            norms_ref[k : k + 1, :] = jnp.sum(mine * mine + other * other, axis=0, keepdims=True)
        else:
            mine = down_ref[...] + got_ref[4]
        low, high = mine[:32, :], mine[32:, :]
        keep_ref[k] = jnp.where(side == 0, low, high)
        send_ref[k] = jnp.where(side == 0, high, low).astype(bf16)


def totals(place, own, down, got):
    width = own.shape[2]
    return pl.pallas_call(
        total_kernel,
        out_shape=(
            jax.ShapeDtypeStruct((3, 32, width), f32),
            jax.ShapeDtypeStruct((3, 32, width), bf16),
            jax.ShapeDtypeStruct((2, width), f32),
        ),
        in_specs=[SMEM, VMEM, VMEM, VMEM],
        out_specs=(VMEM,) * 3,
        compiler_params=pltpu.CompilerParams(vmem_limit_bytes=LIMIT),
        name="totals",
    )(place, own, down, got)


def place_kernel(place_ref, own_ref, got_ref, glu_ref, lin_ref, down_ref, norms_ref):
    side = place_ref[0]
    for k, ref in enumerate((glu_ref, lin_ref, down_ref)):
        for j in range(own_ref.shape[2] // 128):
            cols = slice(128 * j, 128 * j + 128)
            ref[:, block(j, side)] = own_ref[k, :, cols]
            ref[:, block(j, 1 - side)] = got_ref[k, :, cols].astype(f32)
    down, got = own_ref[2], got_ref[2].astype(f32)
    each = jnp.sum(down * down + got * got, axis=1, keepdims=True)
    spread = jnp.where(iota((32, 128), 0) == iota((32, 128), 1), each, 0.0)
    norms_ref[...] = jnp.sum(spread, axis=0, keepdims=True)


def place_grads(place, own, got):
    shape = jax.ShapeDtypeStruct((32, 2 * own.shape[2]), f32)
    return pl.pallas_call(
        place_kernel,
        out_shape=(shape, shape, shape, jax.ShapeDtypeStruct((1, 128), f32)),
        in_specs=[SMEM] + [VMEM] * 2,
        out_specs=(VMEM,) * 4,
        compiler_params=pltpu.CompilerParams(vmem_limit_bytes=LIMIT),
        name="place_grads",
    )(place, own, got)


def combine_kernel(place_ref, routes_ref, back_ref, norms_ref, got_ref, msg_ref):
    experts = back_ref.shape[0]
    height = back_ref.shape[2]
    blocks = (height - 8) // ROWS
    tok = routes_ref.shape[1]
    depth = msg_ref.shape[0]
    key, first = slot_keys(routes_ref[...], experts)
    key2 = jnp.concatenate([key, key], axis=1)
    targets = [slot_target(tok, core * HALF) for core in range(2)]
    picks = jnp.concatenate(
        [
            jnp.where(targets[core] == key2[e : e + 1, :], 1.0, 0.0)
            for e in range(experts)
            for core in range(2)
        ],
        axis=0,
    )
    pick = picks.astype(bf16)
    for q in range(blocks):
        rows = back_ref[:, :, q * ROWS : (q + 1) * ROWS, :].reshape(experts * 2 * ROWS, 128)
        sums = tn(rows, pick).astype(bf16)
        for h in range(2):
            for b in range(2):
                msg_ref[h * (depth // 2) + 2 * q + b, 0:64, :] = sums[
                    64 * b : 64 * b + 64, h * tok : (h + 1) * tok
                ]
    tail = back_ref[:, :, blocks * ROWS :, :].astype(f32).reshape(experts * 2, 8, 128)
    parts = tail[:, 0:1, :] + tail[:, 1:2, :]
    spread = jnp.broadcast_to(parts, (experts * 2, ROWS, 128)).reshape(experts * 2 * ROWS, 128)
    shape = spread.shape
    lanes = iota(shape, 1) == lax.rem(iota(shape, 0), ROWS)
    column = jnp.sum(jnp.where(lanes, spread, 0.0), axis=1, keepdims=True)
    placed = (picks[:, :tok] * column).reshape(experts, 2 * ROWS, tok)
    each = jnp.sum(placed, axis=1)
    named_first = jnp.sum(jnp.where(first, each, 0.0), axis=0, keepdims=True)
    named_second = jnp.sum(jnp.where(first, 0.0, each), axis=0, keepdims=True)
    high_first = named_first.astype(bf16).astype(f32)
    high_second = named_second.astype(bf16).astype(f32)
    row = iota((8, 128), 0)
    gate_rows = jnp.where(row == 0, high_first, jnp.where(row == 1, high_second, 0.0))
    gate_rows = jnp.where(row == 2, named_first - high_first, gate_rows)
    gate_rows = jnp.where(row == 3, named_second - high_second, gate_rows)
    count = norms_ref.shape[1] // 128
    lines = []
    for k in range(2):
        for n in range(count):
            own = norms_ref[k : k + 1, n * 128 : (n + 1) * 128]
            got = got_ref[k : k + 1, n * 128 : (n + 1) * 128]
            lines.append(jnp.where(place_ref[0] == 0, own, got))
            lines.append(jnp.where(place_ref[0] == 0, got, own))
    lines = jnp.concatenate(lines, axis=0)
    extra = jnp.concatenate([lines, gate_rows], axis=0).astype(bf16)
    for z in range(depth):
        msg_ref[z, 64:, :] = extra


def combine(place, routes, back, norms, got, depth):
    height = 64 + 4 * norms.shape[1] // 128 + 8
    return pl.pallas_call(
        combine_kernel,
        out_shape=jax.ShapeDtypeStruct((depth, height, 128), bf16),
        in_specs=[SMEM] + [VMEM] * 4,
        out_specs=VMEM,
        compiler_params=pltpu.CompilerParams(vmem_limit_bytes=LIMIT),
        name="combine",
    )(place, routes, back, norms, got)


def finish_kernel(parts_ref, gates_ref, tok_ref, gate_ref, glu_ref, lin_ref):
    total = jnp.sum(parts_ref[...].astype(f32), axis=0)
    lines = glu_ref.shape[0]
    tok_ref[...] = total[:64, :].astype(bf16)
    glu_ref[...] = total[64 : 64 + lines, :]
    lin_ref[...] = total[64 + lines : 64 + 2 * lines, :]
    tail = total[64 + 2 * lines :, :]
    gate_ref[...] = (tail[0:2, :] + tail[2:4, :]) / gates_ref[...]


def finish(parts, gates):
    lines = (parts.shape[1] - 72) // 2
    return pl.pallas_call(
        finish_kernel,
        out_shape=(
            jax.ShapeDtypeStruct((64, 128), bf16),
            jax.ShapeDtypeStruct((2, 128), f32),
            jax.ShapeDtypeStruct((lines, 128), f32),
            jax.ShapeDtypeStruct((lines, 128), f32),
        ),
        in_specs=[VMEM] * 2,
        out_specs=(VMEM,) * 4,
        compiler_params=pltpu.CompilerParams(vmem_limit_bytes=LIMIT),
        name="finish",
    )(parts, gates)


def over_side(x):
    return lax.ppermute(x, "side", [(0, 1), (1, 0)])


def over_core(x):
    return lax.ppermute(x, "core", [(0, 1), (1, 0)])


def layer(tokens, routes, gates, cotangent, w_glu, w_lin, w_down):
    experts = lax.axis_size("ep")
    depth = lax.axis_size("team")
    _, width = tokens.shape
    place = lax.axis_index("side").astype(jnp.int32).reshape(1)
    core = lax.axis_index("core").astype(jnp.int32).reshape(1)
    routes_t, gates_t = routes.T, gates.T

    packed = pack_rows(place, core, routes_t, gates_t, tokens, cotangent, experts)
    rows = lax.all_to_all(packed.reshape(experts, ROWS, width // 2), "ep", 0, 0, tiled=True)
    rows = rows.reshape(experts * ROWS, width // 2)

    keep, send = part_weights(place, w_glu[0].T, w_lin[0].T, w_down[0])
    got = over_side(send)
    wall, wret = gather_weights(place, keep, got, over_core(keep), over_core(got))

    mine = pre_parts(rows, wall)
    grads, msg = units(mine, over_side(mine), wret)
    msg = msg.reshape(experts * 2, *msg.shape[2:])
    back = lax.all_to_all(msg, ("ep", "core"), 0, 0, tiled=True)
    back = back.reshape(experts, 2, *msg.shape[1:])

    part, down = wgrads(grads, rows)
    own, other, norms = totals(place, part, down, over_core(part))
    norms_got = over_side(norms)
    msg = combine(place, routes_t, back, norms, norms_got, depth)
    parts = lax.all_to_all(msg, "team", 0, 0, tiled=True)
    other, msg = lax.optimization_barrier((other, msg))
    got = over_side(other)
    glu_wg, lin_wg, down_wg, down_norms = place_grads(place, own, got)
    tok_t, gate_t, glu_norms, lin_norms = finish(parts, gates_t)
    return (
        tok_t.T,
        gate_t.T,
        glu_wg.T[None],
        lin_wg.T[None],
        down_wg[None],
        glu_norms.reshape(1, width),
        lin_norms.reshape(1, width),
        down_norms[:, :32],
    )


def solution(mesh):
    teams = mesh.shape["tp"] // 4
    split = Mesh(
        mesh.devices.reshape(mesh.shape["ep"], teams, 2, 2), ("ep", "team", "side", "core")
    )
    tp = ("team", "side", "core")
    return jax.shard_map(
        layer,
        mesh=split,
        in_specs=(
            P("ep", None),
            P("ep", None),
            P("ep", None),
            P("ep", None),
            P("ep", None, tp),
            P("ep", None, tp),
            P("ep", tp, None),
        ),
        out_specs=(
            P("ep", tp),
            P("ep", None),
            P("ep", None, tp),
            P("ep", None, tp),
            P("ep", tp, None),
            P("ep", None),
            P("ep", None),
            P("ep", tp),
        ),
        check_vma=False,
    )
```

```python
import jax
import jax.numpy as jnp
from jax import lax
from jax.experimental import pallas as pl
from jax.experimental.pallas import tpu as pltpu
from jax.sharding import Mesh
from jax.sharding import PartitionSpec as P

clamp_limit = 7.0
sigmoid_scale = 1.702
HALF = 12
LIMIT = 24 * 1024 * 1024
ROWS = 24
f32 = jnp.float32
bf16 = jnp.bfloat16

VMEM = pl.BlockSpec(memory_space=pltpu.VMEM)
SMEM = pl.BlockSpec(memory_space=pltpu.SMEM)


def nt(a, b):
    return lax.dot_general(a, b, (((1,), (1,)), ((), ())), preferred_element_type=f32)


def tn(a, b):
    return lax.dot_general(a, b, (((0,), (0,)), ((), ())), preferred_element_type=f32)


def iota(shape, dim):
    return lax.broadcasted_iota(jnp.int32, shape, dim)


def first_team(teams):
    return teams * 5 // 8


def block(j, side):
    return pl.ds(pl.multiple_of((2 * j + side) * 128, 128), 128)


def slot_keys(routes, experts):
    tok = routes.shape[1]
    e = iota((experts, tok), 0)
    first = jnp.broadcast_to(routes[0:1, :], (experts, tok)) == e
    second = jnp.broadcast_to(routes[1:2, :], (experts, tok)) == e
    named = jnp.where(first | second, 1.0, 0.0)
    before = jnp.where(iota((tok, tok), 0) < iota((tok, tok), 1), 1.0, 0.0).astype(bf16)
    rank = jnp.dot(named.astype(bf16), before, preferred_element_type=f32)
    return jnp.where(named > 0.0, rank, -1.0), first


def slot_target(tok, first_slot):
    r = iota((ROWS, 2 * tok), 0)
    h = jnp.where(iota((ROWS, 2 * tok), 1) >= tok, 1, 0)
    mine = jnp.where(r >= HALF, 1, 0) == h
    return jnp.where(mine, (first_slot + r - HALF * h).astype(f32), -2.0)


def pack_kernel(place_ref, core_ref, routes_ref, gates_ref, tok_ref, cot_ref, out_ref, pick_ref, scale_ref):
    experts = out_ref.shape[0] // ROWS
    tok = tok_ref.shape[0]
    width = out_ref.shape[1]
    side = place_ref[0]
    key, first = slot_keys(routes_ref[...], experts)
    gate = jnp.where(
        first,
        jnp.broadcast_to(gates_ref[0:1, :], key.shape),
        jnp.broadcast_to(gates_ref[1:2, :], key.shape),
    )
    key2 = jnp.concatenate([key, key], axis=1)
    gate2 = jnp.concatenate([jnp.ones_like(gate), gate], axis=1)
    target = slot_target(tok, core_ref[0] * HALF)
    picks = jnp.concatenate(
        [jnp.where(target == key2[e : e + 1, :], 1.0, 0.0) for e in range(experts)], axis=0
    )
    scales = jnp.concatenate(
        [jnp.broadcast_to(gate2[e : e + 1, :], (ROWS, 2 * tok)) for e in range(experts)], axis=0
    )
    scale_ref[...] = jnp.broadcast_to(
        jnp.sum(picks * scales, axis=1, keepdims=True), scale_ref.shape
    )
    pick_ref[...] = picks.astype(bf16)
    wide = min(4, width // 128)

    @pl.loop(0, width // (128 * wide))
    def _(n):
        both = jnp.concatenate(
            [
                jnp.concatenate([ref[:, block(n * wide + k, side)] for k in range(wide)], axis=1)
                for ref in (tok_ref, cot_ref)
            ],
            axis=0,
        )
        rows = jnp.dot(pick_ref[...], both, preferred_element_type=f32)
        scale = jnp.concatenate([scale_ref[...]] * wide, axis=1)
        cols = pl.ds(pl.multiple_of(n * 128 * wide, 128 * wide), 128 * wide)
        out_ref[:, cols] = (rows * scale).astype(bf16)


def pack_rows(place, core, routes, gates, tokens, cotangent, experts):
    tok, width = tokens.shape
    return pl.pallas_call(
        pack_kernel,
        out_shape=jax.ShapeDtypeStruct((experts * ROWS, width // 2), bf16),
        in_specs=[SMEM, SMEM, VMEM, VMEM, VMEM, VMEM],
        out_specs=VMEM,
        scratch_shapes=[
            pltpu.VMEM((experts * ROWS, 2 * tok), bf16),
            pltpu.VMEM((experts * ROWS, 128), f32),
        ],
        name="pack_rows",
    )(place, core, routes, gates, tokens, cotangent)


def part_kernel(place_ref, glu_ref, lin_ref, down_ref, keep_ref, send_ref):
    side = place_ref[0]
    for k, ref in enumerate((glu_ref, lin_ref, down_ref)):
        for j in range(keep_ref.shape[1] // 128):
            cols = slice(128 * j, 128 * j + 128)
            keep_ref[32 * k : 32 * k + 32, cols] = ref[:, block(j, side)]
            send_ref[32 * k : 32 * k + 32, cols] = ref[:, block(j, 1 - side)]


def part_weights(place, glu, lin, down):
    shape = jax.ShapeDtypeStruct((96, glu.shape[1] // 2), bf16)
    return pl.pallas_call(
        part_kernel,
        out_shape=(shape, shape),
        in_specs=[SMEM, VMEM, VMEM, VMEM],
        out_specs=(VMEM,) * 2,
        compiler_params=pltpu.CompilerParams(vmem_limit_bytes=LIMIT),
        name="part_weights",
    )(place, glu, lin, down)


def gather_kernel(place_ref, keep_ref, side_ref, core_ref, cross_ref, wall_ref, wret_ref):
    def fill(order):
        for k in range(3):
            for n, ref in enumerate(order):
                at = 128 * k + 32 * n
                wall_ref[at : at + 32, :] = ref[32 * k : 32 * k + 32, :]

    @pl.when(place_ref[0] == 0)
    def _():
        fill((keep_ref, side_ref, core_ref, cross_ref))

    @pl.when(place_ref[0] == 1)
    def _():
        fill((side_ref, keep_ref, cross_ref, core_ref))

    half = wall_ref.shape[1] // 2
    low = iota((256, 128), 1) < 64
    for h in range(2):
        for q in range(half // 256):
            at = h * half + q * 256
            one = wall_ref[0:256, at : at + 128].astype(f32)
            two = wall_ref[0:256, at + 128 : at + 256].astype(f32)
            even = jnp.where(low, one, pltpu.roll(two, 64, 1))
            odd = jnp.where(low, pltpu.roll(one, 64, 1), two)
            cols = slice(128 * q, 128 * q + 128)
            wret_ref[0, 256 * h : 256 * h + 256, cols] = even.astype(bf16)
            wret_ref[1, 256 * h : 256 * h + 256, cols] = odd.astype(bf16)


def gather_weights(place, keep, side, core, cross):
    width = keep.shape[1]
    return pl.pallas_call(
        gather_kernel,
        out_shape=(
            jax.ShapeDtypeStruct((384, width), bf16),
            jax.ShapeDtypeStruct((2, 512, width // 4), bf16),
        ),
        in_specs=[SMEM] + [VMEM] * 4,
        out_specs=(VMEM,) * 2,
        compiler_params=pltpu.CompilerParams(vmem_limit_bytes=LIMIT),
        name="gather_weights",
    )(place, keep, side, core, cross)


def pre_kernel(rows_ref, wall_ref, out_ref):
    count = rows_ref.shape[0]
    pre = nt(rows_ref[...], wall_ref[...])
    upper = lax.rem(iota((count, 128), 0), ROWS) < HALF
    out_ref[0:count, :] = jnp.where(upper, pre[:, :128], pre[:, 256:])
    lin = pre[:, 128:256].reshape(count // (2 * ROWS), 2, ROWS, 128)
    moved = jnp.roll(pre[:, 128:256], HALF, axis=0).reshape(lin.shape)
    top = iota((count // (2 * ROWS), ROWS, 128), 1) < HALF
    out_ref[count:, :] = jnp.where(top, lin[:, 0], moved[:, 1]).reshape(count // 2, 128)


def pre_parts(rows, wall):
    count = rows.shape[0]
    return pl.pallas_call(
        pre_kernel,
        out_shape=jax.ShapeDtypeStruct((count + count // 2, 128), f32),
        in_specs=[VMEM, VMEM],
        out_specs=VMEM,
        compiler_params=pltpu.CompilerParams(vmem_limit_bytes=LIMIT),
        name="pre_parts",
    )(rows, wall)


def unit_kernel(mine_ref, got_ref, wret_ref, grads_ref, msg_ref):
    count = grads_ref.shape[0]
    sources = count // ROWS
    units = 128
    glu_pre = mine_ref[0:count, :] + got_ref[0:count, :]
    hid_grad = jnp.roll(glu_pre, -HALF, axis=0)
    lin = mine_ref[count:, :] + got_ref[count:, :]
    moved = jnp.roll(lin, -HALF, axis=0)
    lin_pre = jnp.concatenate(
        [lin.reshape(sources // 2, 1, ROWS, units), moved.reshape(sources // 2, 1, ROWS, units)],
        axis=1,
    ).reshape(count, units)
    keep = lax.rem(iota((count, units), 0), ROWS) < HALF
    glu_clip = jnp.minimum(glu_pre, clamp_limit)
    lin_clip = jnp.clip(lin_pre, -clamp_limit, clamp_limit)
    sig = jax.nn.sigmoid(sigmoid_scale * glu_clip)
    glu_act = glu_clip * sig
    hidden = glu_act * (lin_clip + 1.0)
    slope = sig + sigmoid_scale * glu_clip * sig * (1.0 - sig)
    glu_grad = jnp.where(
        keep & (glu_pre < clamp_limit), hid_grad * (lin_clip + 1.0) * slope, 0.0
    )
    lin_grad = jnp.where(keep & (jnp.abs(lin_pre) < clamp_limit), hid_grad * glu_act, 0.0)
    hidden = jnp.where(keep, hidden, 0.0)
    gate_part = jnp.sum(hid_grad * hidden, axis=1, keepdims=True)
    both = jnp.concatenate([glu_grad, lin_grad], axis=1)
    down = jnp.roll(hidden, HALF, axis=0)
    grads_ref[...] = jnp.concatenate([both, down], axis=1).astype(bf16)
    shifted = jnp.roll(both, HALF, axis=0)
    left = jnp.concatenate([both, shifted], axis=1).astype(bf16)
    lanes = iota((count, 128), 1) == lax.rem(iota((count, 128), 0), ROWS)
    spread = jnp.where(lanes, gate_part, 0.0).reshape(sources, ROWS, 128)
    parts = jnp.sum(spread, axis=1, keepdims=True)
    high = parts.astype(bf16).astype(f32)
    row = iota((sources, 8, 128), 1)
    tail = jnp.where(row == 0, high, jnp.where(row == 1, parts - high, 0.0)).astype(bf16)
    blocks = wret_ref.shape[2] // 128
    for core in range(2):
        part = jnp.dot(left, wret_ref[core], preferred_element_type=f32).astype(bf16)
        for q in range(blocks):
            msg_ref[:, core, q * ROWS : (q + 1) * ROWS, :] = part[
                :, q * 128 : (q + 1) * 128
            ].reshape(sources, ROWS, 128)
        msg_ref[:, core, blocks * ROWS :, :] = tail


def units(mine, got, wret):
    count = mine.shape[0] // 3 * 2
    height = wret.shape[2] // 128 * ROWS + 8
    return pl.pallas_call(
        unit_kernel,
        out_shape=(
            jax.ShapeDtypeStruct((count, 384), bf16),
            jax.ShapeDtypeStruct((count // ROWS, 2, height, 128), bf16),
        ),
        in_specs=[VMEM, VMEM, VMEM],
        out_specs=(VMEM, VMEM),
        compiler_params=pltpu.CompilerParams(vmem_limit_bytes=LIMIT),
        name="units",
    )(mine, got, wret)


def wgrad_kernel(grads_ref, rows_ref, part_ref, down_ref):
    step = min(512, rows_ref.shape[1])

    @pl.loop(0, rows_ref.shape[1] // step)
    def _(n):
        cols = pl.ds(pl.multiple_of(n * step, step), step)
        part = tn(grads_ref[...], rows_ref[:, cols])
        for k in range(4):
            part_ref[k, :, cols] = part[64 * k : 64 * k + 64, :]
        down_ref[:, cols] = part[256:320, :]
        part_ref[4, :, cols] = part[320:384, :]


def wgrads(grads, rows):
    width = rows.shape[1]
    return pl.pallas_call(
        wgrad_kernel,
        out_shape=(
            jax.ShapeDtypeStruct((5, 64, width), f32),
            jax.ShapeDtypeStruct((64, width), f32),
        ),
        in_specs=[VMEM, VMEM],
        out_specs=(VMEM,) * 2,
        compiler_params=pltpu.CompilerParams(vmem_limit_bytes=LIMIT),
        name="wgrads",
    )(grads, rows)


def total_kernel(place_ref, own_ref, down_ref, got_ref, keep_ref, send_ref, norms_ref):
    side = place_ref[0]
    for k in range(3):
        if k < 2:
            mine = own_ref[2 * k] + got_ref[2 * k + 1]
            other = own_ref[2 * k + 1] + got_ref[2 * k]
            norms_ref[k : k + 1, :] = jnp.sum(mine * mine + other * other, axis=0, keepdims=True)
        else:
            mine = down_ref[...] + got_ref[4]
        low, high = mine[:32, :], mine[32:, :]
        keep_ref[k] = jnp.where(side == 0, low, high)
        send_ref[k] = jnp.where(side == 0, high, low).astype(bf16)


def totals(place, own, down, got):
    width = own.shape[2]
    return pl.pallas_call(
        total_kernel,
        out_shape=(
            jax.ShapeDtypeStruct((3, 32, width), f32),
            jax.ShapeDtypeStruct((3, 32, width), bf16),
            jax.ShapeDtypeStruct((2, width), f32),
        ),
        in_specs=[SMEM, VMEM, VMEM, VMEM],
        out_specs=(VMEM,) * 3,
        compiler_params=pltpu.CompilerParams(vmem_limit_bytes=LIMIT),
        name="totals",
    )(place, own, down, got)


def place_kernel(place_ref, own_ref, got_ref, glu_ref, lin_ref, down_ref, norms_ref):
    side = place_ref[0]
    for k, ref in enumerate((glu_ref, lin_ref, down_ref)):
        for j in range(own_ref.shape[2] // 128):
            cols = slice(128 * j, 128 * j + 128)
            ref[:, block(j, side)] = own_ref[k, :, cols]
            ref[:, block(j, 1 - side)] = got_ref[k, :, cols].astype(f32)
    down, got = own_ref[2], got_ref[2].astype(f32)
    each = jnp.sum(down * down + got * got, axis=1, keepdims=True)
    spread = jnp.where(iota((32, 128), 0) == iota((32, 128), 1), each, 0.0)
    norms_ref[...] = jnp.sum(spread, axis=0, keepdims=True)


def place_grads(place, own, got):
    shape = jax.ShapeDtypeStruct((32, 2 * own.shape[2]), f32)
    return pl.pallas_call(
        place_kernel,
        out_shape=(shape, shape, shape, jax.ShapeDtypeStruct((1, 128), f32)),
        in_specs=[SMEM] + [VMEM] * 2,
        out_specs=(VMEM,) * 4,
        compiler_params=pltpu.CompilerParams(vmem_limit_bytes=LIMIT),
        name="place_grads",
    )(place, own, got)


def combine_kernel(place_ref, routes_ref, back_ref, norms_ref, got_ref, msg_ref):
    experts = back_ref.shape[0]
    height = back_ref.shape[2]
    blocks = (height - 8) // ROWS
    tok = routes_ref.shape[1]
    depth = msg_ref.shape[0]
    key, first = slot_keys(routes_ref[...], experts)
    key2 = jnp.concatenate([key, key], axis=1)
    targets = [slot_target(tok, core * HALF) for core in range(2)]
    picks = jnp.concatenate(
        [
            jnp.where(targets[core] == key2[e : e + 1, :], 1.0, 0.0)
            for e in range(experts)
            for core in range(2)
        ],
        axis=0,
    )
    pick = picks.astype(bf16)
    for q in range(blocks):
        rows = back_ref[:, :, q * ROWS : (q + 1) * ROWS, :].reshape(experts * 2 * ROWS, 128)
        sums = tn(rows, pick).astype(bf16)
        for h in range(2):
            for b in range(2):
                team = h * (depth // 2) + 2 * q + b
                msg_ref[(team - first_team(depth)) % depth, 0:64, :] = sums[
                    64 * b : 64 * b + 64, h * tok : (h + 1) * tok
                ]
    tail = back_ref[:, :, blocks * ROWS :, :].astype(f32).reshape(experts * 2, 8, 128)
    parts = tail[:, 0:1, :] + tail[:, 1:2, :]
    spread = jnp.broadcast_to(parts, (experts * 2, ROWS, 128)).reshape(experts * 2 * ROWS, 128)
    shape = spread.shape
    lanes = iota(shape, 1) == lax.rem(iota(shape, 0), ROWS)
    column = jnp.sum(jnp.where(lanes, spread, 0.0), axis=1, keepdims=True)
    placed = (picks[:, :tok] * column).reshape(experts, 2 * ROWS, tok)
    each = jnp.sum(placed, axis=1)
    named_first = jnp.sum(jnp.where(first, each, 0.0), axis=0, keepdims=True)
    named_second = jnp.sum(jnp.where(first, 0.0, each), axis=0, keepdims=True)
    high_first = named_first.astype(bf16).astype(f32)
    high_second = named_second.astype(bf16).astype(f32)
    row = iota((8, 128), 0)
    gate_rows = jnp.where(row == 0, high_first, jnp.where(row == 1, high_second, 0.0))
    gate_rows = jnp.where(row == 2, named_first - high_first, gate_rows)
    gate_rows = jnp.where(row == 3, named_second - high_second, gate_rows)
    count = norms_ref.shape[1] // 128
    lines = []
    for k in range(2):
        for n in range(count):
            own = norms_ref[k : k + 1, n * 128 : (n + 1) * 128]
            got = got_ref[k : k + 1, n * 128 : (n + 1) * 128]
            lines.append(jnp.where(place_ref[0] == 0, own, got))
            lines.append(jnp.where(place_ref[0] == 0, got, own))
    lines = jnp.concatenate(lines, axis=0)
    extra = jnp.concatenate([lines, gate_rows], axis=0).astype(bf16)
    for z in range(depth):
        msg_ref[z, 64:, :] = extra


def combine(place, routes, back, norms, got, depth):
    height = 64 + 4 * norms.shape[1] // 128 + 8
    return pl.pallas_call(
        combine_kernel,
        out_shape=jax.ShapeDtypeStruct((depth, height, 128), bf16),
        in_specs=[SMEM] + [VMEM] * 4,
        out_specs=VMEM,
        compiler_params=pltpu.CompilerParams(vmem_limit_bytes=LIMIT),
        name="combine",
    )(place, routes, back, norms, got)


def finish_kernel(parts_ref, gates_ref, tok_ref, gate_ref, glu_ref, lin_ref):
    total = jnp.sum(parts_ref[...].astype(f32), axis=0)
    lines = glu_ref.shape[0]
    tok_ref[...] = total[:64, :].astype(bf16)
    glu_ref[...] = total[64 : 64 + lines, :]
    lin_ref[...] = total[64 + lines : 64 + 2 * lines, :]
    tail = total[64 + 2 * lines :, :]
    gate_ref[...] = (tail[0:2, :] + tail[2:4, :]) / gates_ref[...]


def finish(parts, gates):
    lines = (parts.shape[1] - 72) // 2
    return pl.pallas_call(
        finish_kernel,
        out_shape=(
            jax.ShapeDtypeStruct((64, 128), bf16),
            jax.ShapeDtypeStruct((2, 128), f32),
            jax.ShapeDtypeStruct((lines, 128), f32),
            jax.ShapeDtypeStruct((lines, 128), f32),
        ),
        in_specs=[VMEM] * 2,
        out_specs=(VMEM,) * 4,
        compiler_params=pltpu.CompilerParams(vmem_limit_bytes=LIMIT),
        name="finish",
    )(parts, gates)


def over_side(x):
    return lax.ppermute(x, "side", [(0, 1), (1, 0)])


def over_core(x):
    return lax.ppermute(x, "core", [(0, 1), (1, 0)])


def layer(tokens, routes, gates, cotangent, w_glu, w_lin, w_down):
    experts = lax.axis_size("ep")
    depth = lax.axis_size("team")
    _, width = tokens.shape
    place = lax.axis_index("side").astype(jnp.int32).reshape(1)
    core = lax.axis_index("core").astype(jnp.int32).reshape(1)
    routes_t, gates_t = routes.T, gates.T

    packed = pack_rows(place, core, routes_t, gates_t, tokens, cotangent, experts)
    rows = lax.all_to_all(packed.reshape(experts, ROWS, width // 2), "ep", 0, 0, tiled=True)
    rows = rows.reshape(experts * ROWS, width // 2)

    keep, send = part_weights(place, w_glu[0].T, w_lin[0].T, w_down[0])
    got = over_side(send)
    wall, wret = gather_weights(place, keep, got, over_core(keep), over_core(got))

    mine = pre_parts(rows, wall)
    grads, msg = units(mine, over_side(mine), wret)
    msg = msg.reshape(experts * 2, *msg.shape[2:])
    back = lax.all_to_all(msg, ("ep", "core"), 0, 0, tiled=True)
    back = back.reshape(experts, 2, *msg.shape[1:])

    part, down = wgrads(grads, rows)
    own, other, norms = totals(place, part, down, over_core(part))
    norms_got = over_side(norms)
    msg = combine(place, routes_t, back, norms, norms_got, depth)
    turned = [(n + first_team(depth)) % depth for n in range(depth)]
    parts = lax.all_to_all(msg, "team", 0, 0, axis_index_groups=[turned], tiled=True)
    got = over_side(other)
    glu_wg, lin_wg, down_wg, down_norms = place_grads(place, own, got)
    tok_t, gate_t, glu_norms, lin_norms = finish(parts, gates_t)
    return (
        tok_t.T,
        gate_t.T,
        glu_wg.T[None],
        lin_wg.T[None],
        down_wg[None],
        glu_norms.reshape(1, width),
        lin_norms.reshape(1, width),
        down_norms[:, :32],
    )


def solution(mesh):
    teams = mesh.shape["tp"] // 4
    split = Mesh(
        mesh.devices.reshape(mesh.shape["ep"], teams, 2, 2), ("ep", "team", "side", "core")
    )
    tp = ("team", "side", "core")
    return jax.shard_map(
        layer,
        mesh=split,
        in_specs=(
            P("ep", None),
            P("ep", None),
            P("ep", None),
            P("ep", None),
            P("ep", None, tp),
            P("ep", None, tp),
            P("ep", tp, None),
        ),
        out_specs=(
            P("ep", tp),
            P("ep", None),
            P("ep", None, tp),
            P("ep", None, tp),
            P("ep", tp, None),
            P("ep", None),
            P("ep", None),
            P("ep", tp),
        ),
        check_vma=False,
    )
```

```python
import jax
import jax.numpy as jnp
from jax import lax
from jax.experimental import pallas as pl
from jax.experimental.pallas import tpu as pltpu
from jax.sharding import Mesh
from jax.sharding import PartitionSpec as P

clamp_limit = 7.0
sigmoid_scale = 1.702
HALF = 12
LIMIT = 24 * 1024 * 1024
ROWS = 24
f32 = jnp.float32
bf16 = jnp.bfloat16

VMEM = pl.BlockSpec(memory_space=pltpu.VMEM)
SMEM = pl.BlockSpec(memory_space=pltpu.SMEM)


def nt(a, b):
    return lax.dot_general(a, b, (((1,), (1,)), ((), ())), preferred_element_type=f32)


def tn(a, b):
    return lax.dot_general(a, b, (((0,), (0,)), ((), ())), preferred_element_type=f32)


def iota(shape, dim):
    return lax.broadcasted_iota(jnp.int32, shape, dim)


def first_team(teams):
    return teams * 5 // 8


def block(j, side):
    return pl.ds(pl.multiple_of((2 * j + side) * 128, 128), 128)


def slot_keys(routes, experts):
    tok = routes.shape[1]
    e = iota((experts, tok), 0)
    first = jnp.broadcast_to(routes[0:1, :], (experts, tok)) == e
    second = jnp.broadcast_to(routes[1:2, :], (experts, tok)) == e
    named = jnp.where(first | second, 1.0, 0.0)
    before = jnp.where(iota((tok, tok), 0) < iota((tok, tok), 1), 1.0, 0.0).astype(bf16)
    rank = jnp.dot(named.astype(bf16), before, preferred_element_type=f32)
    return jnp.where(named > 0.0, rank, -1.0), first


def slot_target(tok, first_slot):
    r = iota((ROWS, 2 * tok), 0)
    h = jnp.where(iota((ROWS, 2 * tok), 1) >= tok, 1, 0)
    mine = jnp.where(r >= HALF, 1, 0) == h
    return jnp.where(mine, (first_slot + r - HALF * h).astype(f32), -2.0)


def pack_kernel(place_ref, core_ref, routes_ref, gates_ref, tok_ref, cot_ref, out_ref, pick_ref, scale_ref):
    experts = out_ref.shape[0] // ROWS
    tok = tok_ref.shape[0]
    width = out_ref.shape[1]
    side = place_ref[0]
    key, first = slot_keys(routes_ref[...], experts)
    gate = jnp.where(
        first,
        jnp.broadcast_to(gates_ref[0:1, :], key.shape),
        jnp.broadcast_to(gates_ref[1:2, :], key.shape),
    )
    key2 = jnp.concatenate([key, key], axis=1)
    gate2 = jnp.concatenate([jnp.ones_like(gate), gate], axis=1)
    target = slot_target(tok, core_ref[0] * HALF)
    picks = jnp.concatenate(
        [jnp.where(target == key2[e : e + 1, :], 1.0, 0.0) for e in range(experts)], axis=0
    )
    scales = jnp.concatenate(
        [jnp.broadcast_to(gate2[e : e + 1, :], (ROWS, 2 * tok)) for e in range(experts)], axis=0
    )
    scale_ref[...] = jnp.broadcast_to(
        jnp.sum(picks * scales, axis=1, keepdims=True), scale_ref.shape
    )
    pick_ref[...] = picks.astype(bf16)
    wide = min(4, width // 128)

    @pl.loop(0, width // (128 * wide))
    def _(n):
        both = jnp.concatenate(
            [
                jnp.concatenate([ref[:, block(n * wide + k, side)] for k in range(wide)], axis=1)
                for ref in (tok_ref, cot_ref)
            ],
            axis=0,
        )
        rows = jnp.dot(pick_ref[...], both, preferred_element_type=f32)
        scale = jnp.concatenate([scale_ref[...]] * wide, axis=1)
        cols = pl.ds(pl.multiple_of(n * 128 * wide, 128 * wide), 128 * wide)
        out_ref[:, cols] = (rows * scale).astype(bf16)


def pack_rows(place, core, routes, gates, tokens, cotangent, experts):
    tok, width = tokens.shape
    return pl.pallas_call(
        pack_kernel,
        out_shape=jax.ShapeDtypeStruct((experts * ROWS, width // 2), bf16),
        in_specs=[SMEM, SMEM, VMEM, VMEM, VMEM, VMEM],
        out_specs=VMEM,
        scratch_shapes=[
            pltpu.VMEM((experts * ROWS, 2 * tok), bf16),
            pltpu.VMEM((experts * ROWS, 128), f32),
        ],
        name="pack_rows",
    )(place, core, routes, gates, tokens, cotangent)


def part_kernel(place_ref, glu_ref, lin_ref, down_ref, keep_ref, send_ref):
    side = place_ref[0]
    for k, ref in enumerate((glu_ref, lin_ref, down_ref)):
        for j in range(keep_ref.shape[1] // 128):
            cols = slice(128 * j, 128 * j + 128)
            keep_ref[32 * k : 32 * k + 32, cols] = ref[:, block(j, side)]
            send_ref[32 * k : 32 * k + 32, cols] = ref[:, block(j, 1 - side)]


def part_weights(place, glu, lin, down):
    shape = jax.ShapeDtypeStruct((96, glu.shape[1] // 2), bf16)
    return pl.pallas_call(
        part_kernel,
        out_shape=(shape, shape),
        in_specs=[SMEM, VMEM, VMEM, VMEM],
        out_specs=(VMEM,) * 2,
        compiler_params=pltpu.CompilerParams(vmem_limit_bytes=LIMIT),
        name="part_weights",
    )(place, glu, lin, down)


def gather_kernel(place_ref, keep_ref, side_ref, core_ref, cross_ref, wall_ref, wret_ref):
    def fill(order):
        for k in range(3):
            for n, ref in enumerate(order):
                at = 128 * k + 32 * n
                wall_ref[at : at + 32, :] = ref[32 * k : 32 * k + 32, :]

    @pl.when(place_ref[0] == 0)
    def _():
        fill((keep_ref, side_ref, core_ref, cross_ref))

    @pl.when(place_ref[0] == 1)
    def _():
        fill((side_ref, keep_ref, cross_ref, core_ref))

    half = wall_ref.shape[1] // 2
    low = iota((256, 128), 1) < 64
    for h in range(2):
        for q in range(half // 256):
            at = h * half + q * 256
            one = wall_ref[0:256, at : at + 128].astype(f32)
            two = wall_ref[0:256, at + 128 : at + 256].astype(f32)
            even = jnp.where(low, one, pltpu.roll(two, 64, 1))
            odd = jnp.where(low, pltpu.roll(one, 64, 1), two)
            cols = slice(128 * q, 128 * q + 128)
            wret_ref[0, 256 * h : 256 * h + 256, cols] = even.astype(bf16)
            wret_ref[1, 256 * h : 256 * h + 256, cols] = odd.astype(bf16)


def gather_weights(place, keep, side, core, cross):
    width = keep.shape[1]
    return pl.pallas_call(
        gather_kernel,
        out_shape=(
            jax.ShapeDtypeStruct((384, width), bf16),
            jax.ShapeDtypeStruct((2, 512, width // 4), bf16),
        ),
        in_specs=[SMEM] + [VMEM] * 4,
        out_specs=(VMEM,) * 2,
        compiler_params=pltpu.CompilerParams(vmem_limit_bytes=LIMIT),
        name="gather_weights",
    )(place, keep, side, core, cross)


def pre_kernel(rows_ref, wall_ref, out_ref):
    count = rows_ref.shape[0]
    pre = nt(rows_ref[...], wall_ref[...])
    upper = lax.rem(iota((count, 128), 0), ROWS) < HALF
    out_ref[0:count, :] = jnp.where(upper, pre[:, :128], pre[:, 256:])
    lin = pre[:, 128:256].reshape(count // (2 * ROWS), 2, ROWS, 128)
    moved = jnp.roll(pre[:, 128:256], HALF, axis=0).reshape(lin.shape)
    top = iota((count // (2 * ROWS), ROWS, 128), 1) < HALF
    out_ref[count:, :] = jnp.where(top, lin[:, 0], moved[:, 1]).reshape(count // 2, 128)


def pre_parts(rows, wall):
    count = rows.shape[0]
    return pl.pallas_call(
        pre_kernel,
        out_shape=jax.ShapeDtypeStruct((count + count // 2, 128), f32),
        in_specs=[VMEM, VMEM],
        out_specs=VMEM,
        compiler_params=pltpu.CompilerParams(vmem_limit_bytes=LIMIT),
        name="pre_parts",
    )(rows, wall)


def unit_kernel(mine_ref, got_ref, wret_ref, grads_ref, msg_ref):
    count = grads_ref.shape[0]
    sources = count // ROWS
    units = 128
    glu_pre = mine_ref[0:count, :] + got_ref[0:count, :]
    hid_grad = jnp.roll(glu_pre, -HALF, axis=0)
    lin = mine_ref[count:, :] + got_ref[count:, :]
    moved = jnp.roll(lin, -HALF, axis=0)
    lin_pre = jnp.concatenate(
        [lin.reshape(sources // 2, 1, ROWS, units), moved.reshape(sources // 2, 1, ROWS, units)],
        axis=1,
    ).reshape(count, units)
    keep = lax.rem(iota((count, units), 0), ROWS) < HALF
    glu_clip = jnp.minimum(glu_pre, clamp_limit)
    lin_clip = jnp.clip(lin_pre, -clamp_limit, clamp_limit)
    sig = jax.nn.sigmoid(sigmoid_scale * glu_clip)
    glu_act = glu_clip * sig
    hidden = glu_act * (lin_clip + 1.0)
    slope = sig + sigmoid_scale * glu_clip * sig * (1.0 - sig)
    glu_grad = jnp.where(
        keep & (glu_pre < clamp_limit), hid_grad * (lin_clip + 1.0) * slope, 0.0
    )
    lin_grad = jnp.where(keep & (jnp.abs(lin_pre) < clamp_limit), hid_grad * glu_act, 0.0)
    hidden = jnp.where(keep, hidden, 0.0)
    gate_part = jnp.sum(hid_grad * hidden, axis=1, keepdims=True)
    both = jnp.concatenate([glu_grad, lin_grad], axis=1)
    down = jnp.roll(hidden, HALF, axis=0)
    grads_ref[...] = jnp.concatenate([both, down], axis=1).astype(bf16)
    shifted = jnp.roll(both, HALF, axis=0)
    left = jnp.concatenate([both, shifted], axis=1).astype(bf16)
    lanes = iota((count, 128), 1) == lax.rem(iota((count, 128), 0), ROWS)
    spread = jnp.where(lanes, gate_part, 0.0).reshape(sources, ROWS, 128)
    parts = jnp.sum(spread, axis=1, keepdims=True)
    high = parts.astype(bf16).astype(f32)
    row = iota((sources, 8, 128), 1)
    tail = jnp.where(row == 0, high, jnp.where(row == 1, parts - high, 0.0)).astype(bf16)
    blocks = wret_ref.shape[2] // 128
    for core in range(2):
        part = jnp.dot(left, wret_ref[core], preferred_element_type=f32).astype(bf16)
        for q in range(blocks):
            msg_ref[:, core, q * ROWS : (q + 1) * ROWS, :] = part[
                :, q * 128 : (q + 1) * 128
            ].reshape(sources, ROWS, 128)
        msg_ref[:, core, blocks * ROWS :, :] = tail


def units(mine, got, wret):
    count = mine.shape[0] // 3 * 2
    height = wret.shape[2] // 128 * ROWS + 8
    return pl.pallas_call(
        unit_kernel,
        out_shape=(
            jax.ShapeDtypeStruct((count, 384), bf16),
            jax.ShapeDtypeStruct((count // ROWS, 2, height, 128), bf16),
        ),
        in_specs=[VMEM, VMEM, VMEM],
        out_specs=(VMEM, VMEM),
        compiler_params=pltpu.CompilerParams(vmem_limit_bytes=LIMIT),
        name="units",
    )(mine, got, wret)


def wgrad_kernel(grads_ref, rows_ref, own_ref, down_ref, send_ref):
    step = min(512, rows_ref.shape[1])

    @pl.loop(0, rows_ref.shape[1] // step)
    def _(n):
        cols = pl.ds(pl.multiple_of(n * step, step), step)
        part = tn(grads_ref[...], rows_ref[:, cols])
        for k in range(4):
            own_ref[k, :, cols] = part[64 * k : 64 * k + 64, :]
            send_ref[k, :, cols] = part[64 * k : 64 * k + 64, :].astype(bf16)
        down_ref[:, cols] = part[256:320, :]
        send_ref[4, :, cols] = part[320:384, :].astype(bf16)


def wgrads(grads, rows):
    width = rows.shape[1]
    return pl.pallas_call(
        wgrad_kernel,
        out_shape=(
            jax.ShapeDtypeStruct((4, 64, width), f32),
            jax.ShapeDtypeStruct((64, width), f32),
            jax.ShapeDtypeStruct((5, 64, width), bf16),
        ),
        in_specs=[VMEM, VMEM],
        out_specs=(VMEM,) * 3,
        compiler_params=pltpu.CompilerParams(vmem_limit_bytes=LIMIT),
        name="wgrads",
    )(grads, rows)


def total_kernel(place_ref, own_ref, down_ref, sent_ref, got_ref, keep_ref, send_ref, norms_ref):
    side = place_ref[0]
    for k in range(3):
        if k < 2:
            first, second = got_ref[2 * k].astype(f32), got_ref[2 * k + 1].astype(f32)
            one = sent_ref[2 * k].astype(f32) + second
            two = sent_ref[2 * k + 1].astype(f32) + first
            norms_ref[k : k + 1, :] = jnp.sum(one * one + two * two, axis=0, keepdims=True)
            mine = own_ref[2 * k] + second
        else:
            mine = down_ref[...] + got_ref[4].astype(f32)
        low, high = mine[:32, :], mine[32:, :]
        keep_ref[k] = jnp.where(side == 0, low, high)
        send_ref[k] = jnp.where(side == 0, high, low).astype(bf16)


def totals(place, own, down, sent, got):
    width = own.shape[2]
    return pl.pallas_call(
        total_kernel,
        out_shape=(
            jax.ShapeDtypeStruct((3, 32, width), f32),
            jax.ShapeDtypeStruct((3, 32, width), bf16),
            jax.ShapeDtypeStruct((2, width), f32),
        ),
        in_specs=[SMEM] + [VMEM] * 4,
        out_specs=(VMEM,) * 3,
        compiler_params=pltpu.CompilerParams(vmem_limit_bytes=LIMIT),
        name="totals",
    )(place, own, down, sent, got)


def place_kernel(place_ref, own_ref, got_ref, glu_ref, lin_ref, down_ref, norms_ref):
    side = place_ref[0]
    for k, ref in enumerate((glu_ref, lin_ref, down_ref)):
        for j in range(own_ref.shape[2] // 128):
            cols = slice(128 * j, 128 * j + 128)
            ref[:, block(j, side)] = own_ref[k, :, cols]
            ref[:, block(j, 1 - side)] = got_ref[k, :, cols].astype(f32)
    down, got = own_ref[2], got_ref[2].astype(f32)
    each = jnp.sum(down * down + got * got, axis=1, keepdims=True)
    spread = jnp.where(iota((32, 128), 0) == iota((32, 128), 1), each, 0.0)
    norms_ref[...] = jnp.sum(spread, axis=0, keepdims=True)


def place_grads(place, own, got):
    shape = jax.ShapeDtypeStruct((32, 2 * own.shape[2]), f32)
    return pl.pallas_call(
        place_kernel,
        out_shape=(shape, shape, shape, jax.ShapeDtypeStruct((1, 128), f32)),
        in_specs=[SMEM] + [VMEM] * 2,
        out_specs=(VMEM,) * 4,
        compiler_params=pltpu.CompilerParams(vmem_limit_bytes=LIMIT),
        name="place_grads",
    )(place, own, got)


def combine_kernel(place_ref, routes_ref, back_ref, norms_ref, got_ref, msg_ref):
    experts = back_ref.shape[0]
    height = back_ref.shape[2]
    blocks = (height - 8) // ROWS
    tok = routes_ref.shape[1]
    depth = msg_ref.shape[0]
    key, first = slot_keys(routes_ref[...], experts)
    key2 = jnp.concatenate([key, key], axis=1)
    targets = [slot_target(tok, core * HALF) for core in range(2)]
    picks = jnp.concatenate(
        [
            jnp.where(targets[core] == key2[e : e + 1, :], 1.0, 0.0)
            for e in range(experts)
            for core in range(2)
        ],
        axis=0,
    )
    pick = picks.astype(bf16)
    for q in range(blocks):
        rows = back_ref[:, :, q * ROWS : (q + 1) * ROWS, :].reshape(experts * 2 * ROWS, 128)
        sums = tn(rows, pick).astype(bf16)
        for h in range(2):
            for b in range(2):
                team = h * (depth // 2) + 2 * q + b
                msg_ref[(team - first_team(depth)) % depth, 0:64, :] = sums[
                    64 * b : 64 * b + 64, h * tok : (h + 1) * tok
                ]
    tail = back_ref[:, :, blocks * ROWS :, :].astype(f32).reshape(experts * 2, 8, 128)
    parts = tail[:, 0:1, :] + tail[:, 1:2, :]
    spread = jnp.broadcast_to(parts, (experts * 2, ROWS, 128)).reshape(experts * 2 * ROWS, 128)
    shape = spread.shape
    lanes = iota(shape, 1) == lax.rem(iota(shape, 0), ROWS)
    column = jnp.sum(jnp.where(lanes, spread, 0.0), axis=1, keepdims=True)
    placed = (picks[:, :tok] * column).reshape(experts, 2 * ROWS, tok)
    each = jnp.sum(placed, axis=1)
    named_first = jnp.sum(jnp.where(first, each, 0.0), axis=0, keepdims=True)
    named_second = jnp.sum(jnp.where(first, 0.0, each), axis=0, keepdims=True)
    high_first = named_first.astype(bf16).astype(f32)
    high_second = named_second.astype(bf16).astype(f32)
    row = iota((8, 128), 0)
    gate_rows = jnp.where(row == 0, high_first, jnp.where(row == 1, high_second, 0.0))
    gate_rows = jnp.where(row == 2, named_first - high_first, gate_rows)
    gate_rows = jnp.where(row == 3, named_second - high_second, gate_rows)
    count = norms_ref.shape[1] // 128
    lines = []
    for k in range(2):
        for n in range(count):
            own = norms_ref[k : k + 1, n * 128 : (n + 1) * 128]
            got = got_ref[k : k + 1, n * 128 : (n + 1) * 128]
            lines.append(jnp.where(place_ref[0] == 0, own, got))
            lines.append(jnp.where(place_ref[0] == 0, got, own))
    lines = jnp.concatenate(lines, axis=0)
    extra = jnp.concatenate([lines, gate_rows], axis=0).astype(bf16)
    for z in range(depth):
        msg_ref[z, 64:, :] = extra


def combine(place, routes, back, norms, got, depth):
    height = 64 + 4 * norms.shape[1] // 128 + 8
    return pl.pallas_call(
        combine_kernel,
        out_shape=jax.ShapeDtypeStruct((depth, height, 128), bf16),
        in_specs=[SMEM] + [VMEM] * 4,
        out_specs=VMEM,
        compiler_params=pltpu.CompilerParams(vmem_limit_bytes=LIMIT),
        name="combine",
    )(place, routes, back, norms, got)


def finish_kernel(parts_ref, gates_ref, tok_ref, gate_ref, glu_ref, lin_ref):
    total = jnp.sum(parts_ref[...].astype(f32), axis=0)
    lines = glu_ref.shape[0]
    tok_ref[...] = total[:64, :].astype(bf16)
    glu_ref[...] = total[64 : 64 + lines, :]
    lin_ref[...] = total[64 + lines : 64 + 2 * lines, :]
    tail = total[64 + 2 * lines :, :]
    gate_ref[...] = (tail[0:2, :] + tail[2:4, :]) / gates_ref[...]


def finish(parts, gates):
    lines = (parts.shape[1] - 72) // 2
    return pl.pallas_call(
        finish_kernel,
        out_shape=(
            jax.ShapeDtypeStruct((64, 128), bf16),
            jax.ShapeDtypeStruct((2, 128), f32),
            jax.ShapeDtypeStruct((lines, 128), f32),
            jax.ShapeDtypeStruct((lines, 128), f32),
        ),
        in_specs=[VMEM] * 2,
        out_specs=(VMEM,) * 4,
        compiler_params=pltpu.CompilerParams(vmem_limit_bytes=LIMIT),
        name="finish",
    )(parts, gates)


def over_side(x):
    return lax.ppermute(x, "side", [(0, 1), (1, 0)])


def over_core(x):
    return lax.ppermute(x, "core", [(0, 1), (1, 0)])


def layer(tokens, routes, gates, cotangent, w_glu, w_lin, w_down):
    experts = lax.axis_size("ep")
    depth = lax.axis_size("team")
    _, width = tokens.shape
    place = lax.axis_index("side").astype(jnp.int32).reshape(1)
    core = lax.axis_index("core").astype(jnp.int32).reshape(1)
    routes_t, gates_t = routes.T, gates.T

    packed = pack_rows(place, core, routes_t, gates_t, tokens, cotangent, experts)
    rows = lax.all_to_all(packed.reshape(experts, ROWS, width // 2), "ep", 0, 0, tiled=True)
    rows = rows.reshape(experts * ROWS, width // 2)

    keep, send = part_weights(place, w_glu[0].T, w_lin[0].T, w_down[0])
    got = over_side(send)
    wall, wret = gather_weights(place, keep, got, over_core(keep), over_core(got))

    mine = pre_parts(rows, wall)
    grads, msg = units(mine, over_side(mine), wret)
    msg = msg.reshape(experts * 2, *msg.shape[2:])
    back = lax.all_to_all(msg, ("ep", "core"), 0, 0, tiled=True)
    back = back.reshape(experts, 2, *msg.shape[1:])

    own, down, sent = wgrads(grads, rows)
    own, other, norms = totals(place, own, down, sent, over_core(sent))
    norms_got = over_side(norms)
    msg = combine(place, routes_t, back, norms, norms_got, depth)
    turned = [(n + first_team(depth)) % depth for n in range(depth)]
    parts = lax.all_to_all(msg, "team", 0, 0, axis_index_groups=[turned], tiled=True)
    got = over_side(other)
    glu_wg, lin_wg, down_wg, down_norms = place_grads(place, own, got)
    tok_t, gate_t, glu_norms, lin_norms = finish(parts, gates_t)
    return (
        tok_t.T,
        gate_t.T,
        glu_wg.T[None],
        lin_wg.T[None],
        down_wg[None],
        glu_norms.reshape(1, width),
        lin_norms.reshape(1, width),
        down_norms[:, :32],
    )


def solution(mesh):
    teams = mesh.shape["tp"] // 4
    split = Mesh(
        mesh.devices.reshape(mesh.shape["ep"], teams, 2, 2), ("ep", "team", "side", "core")
    )
    tp = ("team", "side", "core")
    return jax.shard_map(
        layer,
        mesh=split,
        in_specs=(
            P("ep", None),
            P("ep", None),
            P("ep", None),
            P("ep", None),
            P("ep", None, tp),
            P("ep", None, tp),
            P("ep", tp, None),
        ),
        out_specs=(
            P("ep", tp),
            P("ep", None),
            P("ep", None, tp),
            P("ep", None, tp),
            P("ep", tp, None),
            P("ep", None),
            P("ep", None),
            P("ep", tp),
        ),
        check_vma=False,
    )
```

```python
import jax
import jax.numpy as jnp
from jax import lax
from jax.experimental import pallas as pl
from jax.experimental.pallas import tpu as pltpu
from jax.sharding import Mesh
from jax.sharding import PartitionSpec as P

clamp_limit = 7.0
sigmoid_scale = 1.702
HALF = 12
LIMIT = 24 * 1024 * 1024
ROWS = 24
f32 = jnp.float32
bf16 = jnp.bfloat16

VMEM = pl.BlockSpec(memory_space=pltpu.VMEM)
SMEM = pl.BlockSpec(memory_space=pltpu.SMEM)


def nt(a, b):
    return lax.dot_general(a, b, (((1,), (1,)), ((), ())), preferred_element_type=f32)


def tn(a, b):
    return lax.dot_general(a, b, (((0,), (0,)), ((), ())), preferred_element_type=f32)


def iota(shape, dim):
    return lax.broadcasted_iota(jnp.int32, shape, dim)


def first_team(teams):
    return teams * 5 // 8


def block(j, side):
    return pl.ds(pl.multiple_of((2 * j + side) * 128, 128), 128)


def slot_keys(routes, experts):
    tok = routes.shape[1]
    e = iota((experts, tok), 0)
    first = jnp.broadcast_to(routes[0:1, :], (experts, tok)) == e
    second = jnp.broadcast_to(routes[1:2, :], (experts, tok)) == e
    named = jnp.where(first | second, 1.0, 0.0)
    before = jnp.where(iota((tok, tok), 0) < iota((tok, tok), 1), 1.0, 0.0).astype(bf16)
    rank = jnp.dot(named.astype(bf16), before, preferred_element_type=f32)
    return jnp.where(named > 0.0, rank, -1.0), first


def slot_target(tok, first_slot):
    r = iota((ROWS, 2 * tok), 0)
    h = jnp.where(iota((ROWS, 2 * tok), 1) >= tok, 1, 0)
    mine = jnp.where(r >= HALF, 1, 0) == h
    return jnp.where(mine, (first_slot + r - HALF * h).astype(f32), -2.0)


def pack_kernel(place_ref, core_ref, routes_ref, gates_ref, tok_ref, cot_ref, out_ref, pick_ref, scale_ref):
    experts = out_ref.shape[0] // ROWS
    tok = tok_ref.shape[0]
    width = out_ref.shape[1]
    side = place_ref[0]
    key, first = slot_keys(routes_ref[...], experts)
    gate = jnp.where(
        first,
        jnp.broadcast_to(gates_ref[0:1, :], key.shape),
        jnp.broadcast_to(gates_ref[1:2, :], key.shape),
    )
    key2 = jnp.concatenate([key, key], axis=1)
    gate2 = jnp.concatenate([jnp.ones_like(gate), gate], axis=1)
    target = slot_target(tok, core_ref[0] * HALF)
    picks = jnp.concatenate(
        [jnp.where(target == key2[e : e + 1, :], 1.0, 0.0) for e in range(experts)], axis=0
    )
    scales = jnp.concatenate(
        [jnp.broadcast_to(gate2[e : e + 1, :], (ROWS, 2 * tok)) for e in range(experts)], axis=0
    )
    scale_ref[...] = jnp.broadcast_to(
        jnp.sum(picks * scales, axis=1, keepdims=True), scale_ref.shape
    )
    pick_ref[...] = picks.astype(bf16)
    wide = min(4, width // 128)

    @pl.loop(0, width // (128 * wide))
    def _(n):
        both = jnp.concatenate(
            [
                jnp.concatenate([ref[:, block(n * wide + k, side)] for k in range(wide)], axis=1)
                for ref in (tok_ref, cot_ref)
            ],
            axis=0,
        )
        rows = jnp.dot(pick_ref[...], both, preferred_element_type=f32)
        scale = jnp.concatenate([scale_ref[...]] * wide, axis=1)
        cols = pl.ds(pl.multiple_of(n * 128 * wide, 128 * wide), 128 * wide)
        out_ref[:, cols] = (rows * scale).astype(bf16)


def pack_rows(place, core, routes, gates, tokens, cotangent, experts):
    tok, width = tokens.shape
    return pl.pallas_call(
        pack_kernel,
        out_shape=jax.ShapeDtypeStruct((experts * ROWS, width // 2), bf16),
        in_specs=[SMEM, SMEM, VMEM, VMEM, VMEM, VMEM],
        out_specs=VMEM,
        scratch_shapes=[
            pltpu.VMEM((experts * ROWS, 2 * tok), bf16),
            pltpu.VMEM((experts * ROWS, 128), f32),
        ],
        name="pack_rows",
    )(place, core, routes, gates, tokens, cotangent)


def part_kernel(place_ref, glu_ref, lin_ref, down_ref, keep_ref, send_ref):
    side = place_ref[0]
    for k, ref in enumerate((glu_ref, lin_ref, down_ref)):
        for j in range(keep_ref.shape[1] // 128):
            cols = slice(128 * j, 128 * j + 128)
            keep_ref[32 * k : 32 * k + 32, cols] = ref[:, block(j, side)]
            send_ref[32 * k : 32 * k + 32, cols] = ref[:, block(j, 1 - side)]


def part_weights(place, glu, lin, down):
    shape = jax.ShapeDtypeStruct((96, glu.shape[1] // 2), bf16)
    return pl.pallas_call(
        part_kernel,
        out_shape=(shape, shape),
        in_specs=[SMEM, VMEM, VMEM, VMEM],
        out_specs=(VMEM,) * 2,
        compiler_params=pltpu.CompilerParams(vmem_limit_bytes=LIMIT),
        name="part_weights",
    )(place, glu, lin, down)


def gather_kernel(place_ref, keep_ref, side_ref, core_ref, cross_ref, wall_ref, wret_ref):
    def fill(order):
        for k in range(3):
            for n, ref in enumerate(order):
                at = 128 * k + 32 * n
                wall_ref[at : at + 32, :] = ref[32 * k : 32 * k + 32, :]

    @pl.when(place_ref[0] == 0)
    def _():
        fill((keep_ref, side_ref, core_ref, cross_ref))

    @pl.when(place_ref[0] == 1)
    def _():
        fill((side_ref, keep_ref, cross_ref, core_ref))

    half = wall_ref.shape[1] // 2
    low = iota((256, 128), 1) < 64
    for h in range(2):
        for q in range(half // 256):
            at = h * half + q * 256
            one = wall_ref[0:256, at : at + 128].astype(f32)
            two = wall_ref[0:256, at + 128 : at + 256].astype(f32)
            even = jnp.where(low, one, pltpu.roll(two, 64, 1))
            odd = jnp.where(low, pltpu.roll(one, 64, 1), two)
            cols = slice(128 * q, 128 * q + 128)
            wret_ref[0, 256 * h : 256 * h + 256, cols] = even.astype(bf16)
            wret_ref[1, 256 * h : 256 * h + 256, cols] = odd.astype(bf16)


def gather_weights(place, keep, side, core, cross):
    width = keep.shape[1]
    return pl.pallas_call(
        gather_kernel,
        out_shape=(
            jax.ShapeDtypeStruct((384, width), bf16),
            jax.ShapeDtypeStruct((2, 512, width // 4), bf16),
        ),
        in_specs=[SMEM] + [VMEM] * 4,
        out_specs=(VMEM,) * 2,
        compiler_params=pltpu.CompilerParams(vmem_limit_bytes=LIMIT),
        name="gather_weights",
    )(place, keep, side, core, cross)


def paired(values):
    groups = values.shape[0] // (2 * ROWS)
    still = values.reshape(groups, 2, ROWS, 128)
    moved = jnp.roll(values, HALF, axis=0).reshape(groups, 2, ROWS, 128)
    top = iota((groups, ROWS, 128), 1) < HALF
    return jnp.where(top, still[:, 0], moved[:, 1]).reshape(groups * ROWS, 128)


def unpaired(values):
    groups = values.shape[0] // ROWS
    moved = jnp.roll(values, -HALF, axis=0).reshape(groups, 1, ROWS, 128)
    both = jnp.concatenate([values.reshape(groups, 1, ROWS, 128), moved], axis=1)
    return both.reshape(2 * values.shape[0], 128)


def pre_kernel(rows_ref, wall_ref, up_ref, down_ref):
    half = rows_ref.shape[0] // 2
    pre = nt(rows_ref[...], wall_ref[...])
    up_ref[0:half, :] = paired(pre[:, :128])
    up_ref[half:, :] = paired(pre[:, 128:256])
    down_ref[...] = paired(jnp.roll(pre[:, 256:], -HALF, axis=0)).astype(bf16)


def pre_parts(rows, wall):
    count = rows.shape[0]
    return pl.pallas_call(
        pre_kernel,
        out_shape=(
            jax.ShapeDtypeStruct((count, 128), f32),
            jax.ShapeDtypeStruct((count // 2, 128), bf16),
        ),
        in_specs=[VMEM, VMEM],
        out_specs=(VMEM,) * 2,
        compiler_params=pltpu.CompilerParams(vmem_limit_bytes=LIMIT),
        name="pre_parts",
    )(rows, wall)


def unit_kernel(up_ref, up_got_ref, down_ref, down_got_ref, wret_ref, grads_ref, msg_ref):
    count = grads_ref.shape[0]
    sources = count // ROWS
    units = 128
    half = count // 2
    glu_pre = unpaired(up_ref[0:half, :] + up_got_ref[0:half, :])
    lin_pre = unpaired(up_ref[half:, :] + up_got_ref[half:, :])
    hid_grad = unpaired(down_ref[...].astype(f32) + down_got_ref[...].astype(f32))
    keep = lax.rem(iota((count, units), 0), ROWS) < HALF
    glu_clip = jnp.minimum(glu_pre, clamp_limit)
    lin_clip = jnp.clip(lin_pre, -clamp_limit, clamp_limit)
    sig = jax.nn.sigmoid(sigmoid_scale * glu_clip)
    glu_act = glu_clip * sig
    hidden = glu_act * (lin_clip + 1.0)
    slope = sig + sigmoid_scale * glu_clip * sig * (1.0 - sig)
    glu_grad = jnp.where(
        keep & (glu_pre < clamp_limit), hid_grad * (lin_clip + 1.0) * slope, 0.0
    )
    lin_grad = jnp.where(keep & (jnp.abs(lin_pre) < clamp_limit), hid_grad * glu_act, 0.0)
    hidden = jnp.where(keep, hidden, 0.0)
    gate_part = jnp.sum(hid_grad * hidden, axis=1, keepdims=True)
    both = jnp.concatenate([glu_grad, lin_grad], axis=1)
    down = jnp.roll(hidden, HALF, axis=0)
    grads_ref[...] = jnp.concatenate([both, down], axis=1).astype(bf16)
    shifted = jnp.roll(both, HALF, axis=0)
    left = jnp.concatenate([both, shifted], axis=1).astype(bf16)
    lanes = iota((count, 128), 1) == lax.rem(iota((count, 128), 0), ROWS)
    spread = jnp.where(lanes, gate_part, 0.0).reshape(sources, ROWS, 128)
    parts = jnp.sum(spread, axis=1, keepdims=True)
    high = parts.astype(bf16).astype(f32)
    row = iota((sources, 8, 128), 1)
    tail = jnp.where(row == 0, high, jnp.where(row == 1, parts - high, 0.0)).astype(bf16)
    blocks = wret_ref.shape[2] // 128
    for core in range(2):
        part = jnp.dot(left, wret_ref[core], preferred_element_type=f32).astype(bf16)
        for q in range(blocks):
            msg_ref[:, core, q * ROWS : (q + 1) * ROWS, :] = part[
                :, q * 128 : (q + 1) * 128
            ].reshape(sources, ROWS, 128)
        msg_ref[:, core, blocks * ROWS :, :] = tail


def units(up, up_got, down, down_got, wret):
    count = up.shape[0]
    height = wret.shape[2] // 128 * ROWS + 8
    return pl.pallas_call(
        unit_kernel,
        out_shape=(
            jax.ShapeDtypeStruct((count, 384), bf16),
            jax.ShapeDtypeStruct((count // ROWS, 2, height, 128), bf16),
        ),
        in_specs=[VMEM] * 5,
        out_specs=(VMEM, VMEM),
        compiler_params=pltpu.CompilerParams(vmem_limit_bytes=LIMIT),
        name="units",
    )(up, up_got, down, down_got, wret)


def wgrad_kernel(grads_ref, rows_ref, own_ref, down_ref, send_ref):
    step = min(512, rows_ref.shape[1])

    @pl.loop(0, rows_ref.shape[1] // step)
    def _(n):
        cols = pl.ds(pl.multiple_of(n * step, step), step)
        part = tn(grads_ref[...], rows_ref[:, cols])
        for k in range(4):
            own_ref[k, :, cols] = part[64 * k : 64 * k + 64, :]
            send_ref[k, :, cols] = part[64 * k : 64 * k + 64, :].astype(bf16)
        down_ref[:, cols] = part[256:320, :]
        send_ref[4, :, cols] = part[320:384, :].astype(bf16)


def wgrads(grads, rows):
    width = rows.shape[1]
    return pl.pallas_call(
        wgrad_kernel,
        out_shape=(
            jax.ShapeDtypeStruct((4, 64, width), f32),
            jax.ShapeDtypeStruct((64, width), f32),
            jax.ShapeDtypeStruct((5, 64, width), bf16),
        ),
        in_specs=[VMEM, VMEM],
        out_specs=(VMEM,) * 3,
        compiler_params=pltpu.CompilerParams(vmem_limit_bytes=LIMIT),
        name="wgrads",
    )(grads, rows)


def total_kernel(place_ref, own_ref, down_ref, sent_ref, got_ref, keep_ref, send_ref, norms_ref):
    side = place_ref[0]
    for k in range(3):
        if k < 2:
            first, second = got_ref[2 * k].astype(f32), got_ref[2 * k + 1].astype(f32)
            one = sent_ref[2 * k].astype(f32) + second
            two = sent_ref[2 * k + 1].astype(f32) + first
            norms_ref[k : k + 1, :] = jnp.sum(one * one + two * two, axis=0, keepdims=True)
            mine = own_ref[2 * k] + second
        else:
            mine = down_ref[...] + got_ref[4].astype(f32)
        low, high = mine[:32, :], mine[32:, :]
        keep_ref[k] = jnp.where(side == 0, low, high)
        send_ref[k] = jnp.where(side == 0, high, low).astype(bf16)


def totals(place, own, down, sent, got):
    width = own.shape[2]
    return pl.pallas_call(
        total_kernel,
        out_shape=(
            jax.ShapeDtypeStruct((3, 32, width), f32),
            jax.ShapeDtypeStruct((3, 32, width), bf16),
            jax.ShapeDtypeStruct((2, width), f32),
        ),
        in_specs=[SMEM] + [VMEM] * 4,
        out_specs=(VMEM,) * 3,
        compiler_params=pltpu.CompilerParams(vmem_limit_bytes=LIMIT),
        name="totals",
    )(place, own, down, sent, got)


def place_kernel(place_ref, own_ref, got_ref, glu_ref, lin_ref, down_ref, norms_ref):
    side = place_ref[0]
    for k, ref in enumerate((glu_ref, lin_ref, down_ref)):
        for j in range(own_ref.shape[2] // 128):
            cols = slice(128 * j, 128 * j + 128)
            ref[:, block(j, side)] = own_ref[k, :, cols]
            ref[:, block(j, 1 - side)] = got_ref[k, :, cols].astype(f32)
    down, got = own_ref[2], got_ref[2].astype(f32)
    each = jnp.sum(down * down + got * got, axis=1, keepdims=True)
    spread = jnp.where(iota((32, 128), 0) == iota((32, 128), 1), each, 0.0)
    norms_ref[...] = jnp.sum(spread, axis=0, keepdims=True)


def place_grads(place, own, got):
    shape = jax.ShapeDtypeStruct((32, 2 * own.shape[2]), f32)
    return pl.pallas_call(
        place_kernel,
        out_shape=(shape, shape, shape, jax.ShapeDtypeStruct((1, 128), f32)),
        in_specs=[SMEM] + [VMEM] * 2,
        out_specs=(VMEM,) * 4,
        compiler_params=pltpu.CompilerParams(vmem_limit_bytes=LIMIT),
        name="place_grads",
    )(place, own, got)


def combine_kernel(place_ref, routes_ref, back_ref, norms_ref, got_ref, msg_ref):
    experts = back_ref.shape[0]
    height = back_ref.shape[2]
    blocks = (height - 8) // ROWS
    tok = routes_ref.shape[1]
    depth = msg_ref.shape[0]
    key, first = slot_keys(routes_ref[...], experts)
    key2 = jnp.concatenate([key, key], axis=1)
    targets = [slot_target(tok, core * HALF) for core in range(2)]
    picks = jnp.concatenate(
        [
            jnp.where(targets[core] == key2[e : e + 1, :], 1.0, 0.0)
            for e in range(experts)
            for core in range(2)
        ],
        axis=0,
    )
    pick = picks.astype(bf16)
    for q in range(blocks):
        rows = back_ref[:, :, q * ROWS : (q + 1) * ROWS, :].reshape(experts * 2 * ROWS, 128)
        sums = tn(rows, pick).astype(bf16)
        for h in range(2):
            for b in range(2):
                team = h * (depth // 2) + 2 * q + b
                msg_ref[(team - first_team(depth)) % depth, 0:64, :] = sums[
                    64 * b : 64 * b + 64, h * tok : (h + 1) * tok
                ]
    tail = back_ref[:, :, blocks * ROWS :, :].astype(f32).reshape(experts * 2, 8, 128)
    parts = tail[:, 0:1, :] + tail[:, 1:2, :]
    spread = jnp.broadcast_to(parts, (experts * 2, ROWS, 128)).reshape(experts * 2 * ROWS, 128)
    shape = spread.shape
    lanes = iota(shape, 1) == lax.rem(iota(shape, 0), ROWS)
    column = jnp.sum(jnp.where(lanes, spread, 0.0), axis=1, keepdims=True)
    placed = (picks[:, :tok] * column).reshape(experts, 2 * ROWS, tok)
    each = jnp.sum(placed, axis=1)
    named_first = jnp.sum(jnp.where(first, each, 0.0), axis=0, keepdims=True)
    named_second = jnp.sum(jnp.where(first, 0.0, each), axis=0, keepdims=True)
    high_first = named_first.astype(bf16).astype(f32)
    high_second = named_second.astype(bf16).astype(f32)
    row = iota((8, 128), 0)
    gate_rows = jnp.where(row == 0, high_first, jnp.where(row == 1, high_second, 0.0))
    gate_rows = jnp.where(row == 2, named_first - high_first, gate_rows)
    gate_rows = jnp.where(row == 3, named_second - high_second, gate_rows)
    count = norms_ref.shape[1] // 128
    lines = []
    for k in range(2):
        for n in range(count):
            own = norms_ref[k : k + 1, n * 128 : (n + 1) * 128]
            got = got_ref[k : k + 1, n * 128 : (n + 1) * 128]
            lines.append(jnp.where(place_ref[0] == 0, own, got))
            lines.append(jnp.where(place_ref[0] == 0, got, own))
    lines = jnp.concatenate(lines, axis=0)
    extra = jnp.concatenate([lines, gate_rows], axis=0).astype(bf16)
    for z in range(depth):
        msg_ref[z, 64:, :] = extra


def combine(place, routes, back, norms, got, depth):
    height = 64 + 4 * norms.shape[1] // 128 + 8
    return pl.pallas_call(
        combine_kernel,
        out_shape=jax.ShapeDtypeStruct((depth, height, 128), bf16),
        in_specs=[SMEM] + [VMEM] * 4,
        out_specs=VMEM,
        compiler_params=pltpu.CompilerParams(vmem_limit_bytes=LIMIT),
        name="combine",
    )(place, routes, back, norms, got)


def finish_kernel(parts_ref, gates_ref, tok_ref, gate_ref, glu_ref, lin_ref):
    total = jnp.sum(parts_ref[...].astype(f32), axis=0)
    lines = glu_ref.shape[0]
    tok_ref[...] = total[:64, :].astype(bf16)
    glu_ref[...] = total[64 : 64 + lines, :]
    lin_ref[...] = total[64 + lines : 64 + 2 * lines, :]
    tail = total[64 + 2 * lines :, :]
    gate_ref[...] = (tail[0:2, :] + tail[2:4, :]) / gates_ref[...]


def finish(parts, gates):
    lines = (parts.shape[1] - 72) // 2
    return pl.pallas_call(
        finish_kernel,
        out_shape=(
            jax.ShapeDtypeStruct((64, 128), bf16),
            jax.ShapeDtypeStruct((2, 128), f32),
            jax.ShapeDtypeStruct((lines, 128), f32),
            jax.ShapeDtypeStruct((lines, 128), f32),
        ),
        in_specs=[VMEM] * 2,
        out_specs=(VMEM,) * 4,
        compiler_params=pltpu.CompilerParams(vmem_limit_bytes=LIMIT),
        name="finish",
    )(parts, gates)


def over_side(x):
    return lax.ppermute(x, "side", [(0, 1), (1, 0)])


def over_core(x):
    return lax.ppermute(x, "core", [(0, 1), (1, 0)])


def layer(tokens, routes, gates, cotangent, w_glu, w_lin, w_down):
    experts = lax.axis_size("ep")
    depth = lax.axis_size("team")
    _, width = tokens.shape
    place = lax.axis_index("side").astype(jnp.int32).reshape(1)
    core = lax.axis_index("core").astype(jnp.int32).reshape(1)
    routes_t, gates_t = routes.T, gates.T

    packed = pack_rows(place, core, routes_t, gates_t, tokens, cotangent, experts)
    rows = lax.all_to_all(packed.reshape(experts, ROWS, width // 2), "ep", 0, 0, tiled=True)
    rows = rows.reshape(experts * ROWS, width // 2)

    keep, send = part_weights(place, w_glu[0].T, w_lin[0].T, w_down[0])
    got = over_side(send)
    wall, wret = gather_weights(place, keep, got, over_core(keep), over_core(got))

    up, down = pre_parts(rows, wall)
    up_got = over_side(up)
    down_got = over_side(down)
    grads, msg = units(up, up_got, down, down_got, wret)
    msg = msg.reshape(experts * 2, *msg.shape[2:])
    back = lax.all_to_all(msg, ("ep", "core"), 0, 0, tiled=True)
    back = back.reshape(experts, 2, *msg.shape[1:])

    own, down, sent = wgrads(grads, rows)
    own, other, norms = totals(place, own, down, sent, over_core(sent))
    norms_got = over_side(norms)
    msg = combine(place, routes_t, back, norms, norms_got, depth)
    turned = [(n + first_team(depth)) % depth for n in range(depth)]
    parts = lax.all_to_all(msg, "team", 0, 0, axis_index_groups=[turned], tiled=True)
    got = over_side(other)
    glu_wg, lin_wg, down_wg, down_norms = place_grads(place, own, got)
    tok_t, gate_t, glu_norms, lin_norms = finish(parts, gates_t)
    return (
        tok_t.T,
        gate_t.T,
        glu_wg.T[None],
        lin_wg.T[None],
        down_wg[None],
        glu_norms.reshape(1, width),
        lin_norms.reshape(1, width),
        down_norms[:, :32],
    )


def solution(mesh):
    teams = mesh.shape["tp"] // 4
    split = Mesh(
        mesh.devices.reshape(mesh.shape["ep"], teams, 2, 2), ("ep", "team", "side", "core")
    )
    tp = ("team", "side", "core")
    return jax.shard_map(
        layer,
        mesh=split,
        in_specs=(
            P("ep", None),
            P("ep", None),
            P("ep", None),
            P("ep", None),
            P("ep", None, tp),
            P("ep", None, tp),
            P("ep", tp, None),
        ),
        out_specs=(
            P("ep", tp),
            P("ep", None),
            P("ep", None, tp),
            P("ep", None, tp),
            P("ep", tp, None),
            P("ep", None),
            P("ep", None),
            P("ep", tp),
        ),
        check_vma=False,
    )
```
